32 devices in a mesh: grp: 2 (over x), ep: 8 (over z, y), tp: 2 (over core).
Axes of the slice: x: 2, y: 2, z: 4, core: 2. Of those that a mesh axis runs over, the one named last changes fastest.
Arguments:
- tokens: bfloat16 [2304, 2048], P(('grp', 'ep')), parts along dimension 0, may hold values from -6 to 6
- norm_gain: bfloat16 [2048], replicated, may hold values from 0.099609375 to 1.8984375
- chosen_rows: int32 [16, 144], P('grp', 'ep'), parts along dimension 0, may hold values from 0 to 1151, as said below
- route_weights: float32 [16, 144], P('grp', 'ep'), parts along dimension 0, may hold values from 0.2 to 1
- gate_weight: bfloat16 [8, 2048, 1536], P('ep', None, 'tp'), may hold values from -0.125 to 0.125
- up_weight: bfloat16 [8, 2048, 1536], P('ep', None, 'tp'), may hold values from -0.125 to 0.125
- down_weight: bfloat16 [8, 1536, 2048], P('ep', 'tp'), may hold values from -0.15625 to 0.15625
Outputs:
- mixed: bfloat16 [2304, 2048], P(('grp', 'ep', 'tp')), parts along dimension 0
The draws below stay inside these ranges and needn't reach their ends.
There are 2 independent parts, one for each index of `grp`. The reference program is written for one: setup_inputs(seed, part) draws one part's arguments, and reference() takes and returns one part's arrays. A program takes and returns all parts, laid end to end along the dimension named above; an argument that names none is the same for every part. Nothing has to cross between parts.
Inputs may be any that keep to these rules, and one draw needn't show every extreme that they name: `chosen_rows`: the columns come in blocks of 18, one block for each index of ep's 144 tokens in order. In every row the first half of a block names distinct tokens of the first half of that block's tokens, and its second half distinct tokens of the second half.
All inputs are finite; a program needn't handle non-finite values.
Results may differ from the reference program's by a relative error of at most 0.01.
Values may be sent and summed in bfloat16 or wider, within the bound.
No kernel may reach another device: no remote copies, remote signals or barrier semaphores. Data moves between devices by JAX's collectives and lax.ppermute only.
A program may use at most 128 MiB of HBM per device.

```python
import jax
import jax.numpy as jnp
from jax import lax

D = 2048
FF = 1536
TOK_DEV = 144
EXPERTS = 8
TOKENS = 1152
SLOTS = 18
CAP = 144
N_TP = 2


def draw_chosen_rows(key, part):
    sources = CAP // SLOTS
    half_rows = TOK_DEV // 2
    half_slots = SLOTS // 2
    scores = jax.random.randint(jax.random.fold_in(key, 11), (EXPERTS, sources, 2, half_rows), 0, 1048576)
    scores = scores * half_rows + jnp.arange(half_rows, dtype=jnp.int32)
    order = jnp.argsort(scores, axis=-1, stable=True)[..., :half_slots].astype(jnp.int32)
    source_ids = jnp.arange(sources, dtype=jnp.int32)[None, :, None, None] * TOK_DEV
    half_ids = jnp.arange(2, dtype=jnp.int32)[None, None, :, None] * half_rows
    rows = order + source_ids + half_ids
    return rows.reshape(EXPERTS, CAP).astype(jnp.int32)


def steps_of(rng, extent, shards, low, largest):
    loudness, own = 1.0, jax.random.fold_in(rng, 6)
    for dim, parts in shards:
        heights = jnp.exp(jax.random.uniform(jax.random.fold_in(own, dim), (parts,), jnp.float32, low / len(shards), largest / len(shards)))
        loudness = loudness * jnp.repeat(heights, extent[dim] // parts).reshape([-1 if axis == dim else 1 for axis in range(len(extent))])
    return loudness


def noise(rng, shape, deviation, most, shards=(), kind=jnp.bfloat16):
    result = deviation * jax.random.normal(rng, shape, jnp.float32)
    if shards:
        result = result * steps_of(rng, shape, shards, -0.22, 0.18)
    return jnp.clip(result, -most, most).astype(kind)


def setup_inputs(seed: int = 0, part: int = 0) -> dict:
    arg_keys = jax.random.split(jax.random.key(seed), 8)
    part_splits = jax.random.split(jax.random.fold_in(arg_keys[7], part), 8)
    return {
        "tokens": noise(part_splits[0], (TOKENS, D), 1.0, 6.0, ((0, 8),)),
        "norm_gain": jnp.clip(1.0 + 0.18 * jax.random.normal(arg_keys[1], (D,), jnp.float32), 0.099609375, 1.8984375).astype(jnp.bfloat16),
        "chosen_rows": draw_chosen_rows(jax.random.fold_in(jax.random.fold_in(arg_keys[7], part), 71), part),
        "route_weights": jnp.clip(0.2 + 0.8 * jax.random.uniform(part_splits[3], (EXPERTS, CAP), jnp.float32) ** steps_of(part_splits[3], (EXPERTS, CAP), ((1, 8),), -0.2, 0.2), 0.2, 1.0),
        "gate_weight": noise(arg_keys[4], (EXPERTS, D, FF), D ** -0.5, 0.125, ((0, 8), (2, 2))),
        "up_weight": noise(arg_keys[5], (EXPERTS, D, FF), D ** -0.5, 0.125, ((0, 8), (2, 2))),
        "down_weight": noise(arg_keys[6], (EXPERTS, FF, D), FF ** -0.5, 0.15625, ((0, 8), (1, 2))),
    }


def reference(tokens, norm_gain, chosen_rows, route_weights, gate_weight, up_weight, down_weight):
    values = tokens.astype(jnp.float32)
    scale = lax.rsqrt(lax.optimization_barrier(jnp.mean(values * values, axis=-1, keepdims=True)) + 1e-06)
    normed = (values * scale * norm_gain.astype(jnp.float32)).astype(jnp.bfloat16)
    half_ff = FF // N_TP

    def one_expert(total, inputs):
        expert_rows, expert_weights, w_gate, w_up, w_down = inputs
        expert_in = normed[expert_rows]
        gate_proj = jnp.dot(expert_in, w_gate, preferred_element_type=jnp.float32)
        up_proj = jnp.dot(expert_in, w_up, preferred_element_type=jnp.float32)
        hidden = (jax.nn.silu(gate_proj) * up_proj).astype(jnp.bfloat16)
        summed = jnp.zeros((expert_rows.shape[0], D), jnp.float32)
        for part_id in range(N_TP):
            partial_out = jnp.dot(hidden[:, part_id * half_ff:(part_id + 1) * half_ff], w_down[part_id * half_ff:(part_id + 1) * half_ff], preferred_element_type=jnp.float32).astype(jnp.bfloat16)
            partial_out = lax.optimization_barrier(partial_out)
            summed = summed + partial_out.astype(jnp.float32)
        expert_out = summed.astype(jnp.bfloat16)
        total = total.at[expert_rows].add(expert_weights[:, None] * expert_out.astype(jnp.float32))
        return (total, None)
    start_total = jnp.zeros((TOKENS, D), jnp.float32)
    total, unused = lax.scan(one_expert, start_total, (chosen_rows.astype(jnp.int32), route_weights, gate_weight, up_weight, down_weight))
    return total.astype(jnp.bfloat16)
```

```python
import functools

import jax
import jax.numpy as jnp
from jax import lax
from jax.experimental import pallas as pl
from jax.experimental.pallas import tpu as pltpu
from jax.sharding import PartitionSpec as P

LANES = 128
SUB = 8
F32 = jnp.float32
BF16 = jnp.bfloat16
VMEM = pl.BlockSpec(memory_space=pltpu.VMEM)


def cdiv(a, b):
    return (a + b - 1) // b


def pick(values, wanted):
    lane = lax.broadcasted_iota(jnp.int32, values.shape, 1)
    return jnp.sum(jnp.where(lane == wanted, values, 0.0), axis=1, keepdims=True)


def main_slots(n_main, half_slots, slots):
    sub = lax.broadcasted_iota(jnp.int32, (2 * n_main, slots), 0)
    return jnp.where(sub < n_main, sub, sub - n_main + half_slots)


def dispatch_kernel(tok_ref, gain_ref, rows_ref, out_ref, norm_scr, tail_scr):
    tok_rows, width = tok_ref.shape
    n_dest, slots = rows_ref.shape
    half_slots = slots // 2
    n_main = half_slots // SUB * SUB
    n_tail = half_slots - n_main
    half_width = width // 2
    blocks = half_width // LANES
    core = lax.axis_index("tp")
    base = pl.multiple_of(core * half_width, half_width)
    gain = gain_ref[:, pl.ds(base, half_width)].astype(F32)
    step = 16
    for at in range(0, tok_rows, step):
        rows = slice(at, at + step)
        values = tok_ref[rows, :].astype(F32)
        scale = lax.rsqrt(jnp.mean(values * values, axis=-1, keepdims=True) + 1e-06)
        part = tok_ref[rows, pl.ds(base, half_width)].astype(F32)
        norm_scr[rows, :] = (part * scale * gain).astype(BF16)
    normed = norm_scr[...]
    index = (rows_ref[...] - lax.axis_index("ep") * tok_rows).astype(F32)
    wanted = main_slots(n_main, half_slots, slots)
    group = 2 * n_main

    def one_hot(column):
        token = lax.broadcasted_iota(jnp.int32, (column.shape[0], tok_rows), 1)
        return jnp.where(token == column.astype(jnp.int32), 1.0, 0.0).astype(BF16)

    def chosen(column):
        return jnp.dot(one_hot(column), normed, preferred_element_type=F32)

    for first in range(0, n_dest, SUB):
        columns = [
            pick(jnp.broadcast_to(index[d : d + 1, :], (group, slots)), wanted)
            for d in range(first, first + SUB)
        ]
        got = chosen(jnp.concatenate(columns, axis=0))
        for d in range(SUB):
            for j in range(blocks):
                out_ref[first + d, j * group : (j + 1) * group, :] = got[
                    d * group : (d + 1) * group, j * LANES : (j + 1) * LANES
                ].astype(BF16)
    per_dest = 2 * n_tail * blocks
    columns = [
        pick(index, jnp.full((n_dest, slots), h * half_slots + n_main + t, jnp.int32))
        for h in range(2)
        for t in range(n_tail)
    ]
    got = chosen(jnp.concatenate(columns, axis=0))
    for k in range(2 * n_tail):
        for j in range(blocks):
            tail_scr[pl.ds(k * blocks + j, n_dest, stride=per_dest), :] = got[
                k * n_dest : (k + 1) * n_dest, j * LANES : (j + 1) * LANES
            ]
    for d in range(n_dest):
        out_ref[d, group * blocks :, :] = tail_scr[d * per_dest : (d + 1) * per_dest, :].astype(BF16)


def expert_kernel(
    mine_ref, other_ref, gate_ref, up_ref, down_ref, send_ref, keep_ref,
    x_scr, hidden_scr, tail_scr, back_scr, *, n_main, n_tail,
):
    n_src = mine_ref.shape[0]
    _, width, hidden = gate_ref.shape
    half_width = width // 2
    blocks = half_width // LANES
    group = 2 * n_main
    per_src = 2 * n_tail * blocks
    main_rows = n_src * group
    core = lax.axis_index("tp")
    for ref, base in ((mine_ref, core * half_width), (other_ref, (1 - core) * half_width)):
        for s in range(n_src):
            tail_scr[s * per_src : (s + 1) * per_src, :] = ref[s, group * blocks :, :].astype(F32)
        for j in range(blocks):
            lanes = pl.ds(pl.multiple_of(base + j * LANES, LANES), LANES)
            for s in range(n_src):
                x_scr[s * group : (s + 1) * group, lanes] = ref[s, j * group : (j + 1) * group, :]
            rest = [
                tail_scr[pl.ds(k * blocks + j, n_src, stride=per_src), :] for k in range(2 * n_tail)
            ]
            x_scr[main_rows:, lanes] = jnp.concatenate(rest, axis=0).astype(BF16)
    chunk = 2 * LANES
    x = x_scr[...]
    for at in range(0, hidden, chunk):
        cols = slice(at, at + chunk)
        gate = jnp.dot(x, gate_ref[0, :, cols], preferred_element_type=F32)
        up = jnp.dot(x, up_ref[0, :, cols], preferred_element_type=F32)
        hidden_scr[:, cols] = (gate / (1.0 + jnp.exp(-gate)) * up).astype(BF16)
    act = hidden_scr[...]
    first = core == 0
    all_blocks = width // LANES
    per_back = n_tail * all_blocks
    for at in range(0, width, chunk):
        part = jnp.dot(act, down_ref[0, :, at : at + chunk], preferred_element_type=F32)
        j = at // LANES
        for s in range(n_src):
            halves = []
            for h in range(2):
                row = s * group + h * n_main
                halves.append(
                    jnp.concatenate(
                        [part[row : row + n_main, :LANES], part[row : row + n_main, LANES:]], axis=0
                    )
                )
            place = slice(j * n_main, (j + 2) * n_main)
            send_ref[s, place, :] = jnp.where(first, halves[1], halves[0]).astype(BF16)
            keep_ref[s, place, :] = jnp.where(first, halves[0], halves[1]).astype(BF16)
        for b in range(2):
            lanes = slice(b * LANES, (b + 1) * LANES)
            for t in range(n_tail):
                rows = [main_rows + (h * n_tail + t) * n_src for h in range(2)]
                low, high = (part[row : row + n_src, lanes] for row in rows)
                where = pl.ds(t * all_blocks + j + b, n_src, stride=per_back)
                back_scr[0, where, :] = jnp.where(first, high, low)
                back_scr[1, where, :] = jnp.where(first, low, high)
    for s in range(n_src):
        rows = slice(s * per_back, (s + 1) * per_back)
        send_ref[s, n_main * all_blocks :, :] = back_scr[0, rows, :].astype(BF16)
        keep_ref[s, n_main * all_blocks :, :] = back_scr[1, rows, :].astype(BF16)


def combine_kernel(back_ref, rows_ref, weight_ref, out_ref, row_scr, tail_scr):
    n_exp, slots = rows_ref.shape
    half_slots = slots // 2
    n_main = half_slots // SUB * SUB
    n_tail = half_slots - n_main
    out_rows, width = out_ref.shape
    all_blocks = width // LANES
    per_back = n_tail * all_blocks
    main_rows = n_exp * n_main
    core = lax.axis_index("tp")
    start = lax.axis_index("ep") * (2 * out_rows) + core * out_rows
    index = (rows_ref[...] - start).astype(F32)
    weight = weight_ref[...]
    lane0 = core * half_slots
    wanted = lax.broadcasted_iota(jnp.int32, (n_main, slots), 0) + lane0
    pieces = []

    def entry(idx, wgt):
        token = lax.broadcasted_iota(jnp.int32, (idx.shape[0], cdiv(out_rows, LANES) * LANES), 1)
        return jnp.where(token == idx.astype(jnp.int32), wgt, 0.0)

    for e in range(n_exp):
        columns = [
            pick(jnp.broadcast_to(v[e : e + 1, :], (n_main, slots)), wanted) for v in (index, weight)
        ]
        pieces.append(entry(*columns))
    for t in range(n_tail):
        at = jnp.full((n_exp, slots), n_main + t, jnp.int32) + lane0
        pieces.append(entry(pick(index, at), pick(weight, at)))
    total = n_exp * half_slots
    padded = cdiv(total, LANES) * LANES
    if padded > total:
        pieces.append(jnp.zeros((padded - total, pieces[0].shape[1]), F32))
    spread = jnp.concatenate(pieces, axis=0).T[:out_rows, :]
    high = spread.astype(BF16)
    rest = spread - high.astype(F32)
    mid = rest.astype(BF16)
    low = (rest - mid.astype(F32)).astype(BF16)
    left = jnp.concatenate([high, mid, low], axis=0)
    for e in range(n_exp):
        tail_scr[e * per_back : (e + 1) * per_back, :] = back_ref[e, n_main * all_blocks :, :].astype(F32)
        for j in range(0, all_blocks, 2):
            two = back_ref[e, j * n_main : (j + 2) * n_main, :].astype(F32)
            row_scr[e * n_main : (e + 1) * n_main, j * LANES : (j + 1) * LANES] = two[:n_main]
            row_scr[e * n_main : (e + 1) * n_main, (j + 1) * LANES : (j + 2) * LANES] = two[n_main:]
    for t in range(n_tail):
        rows = slice(main_rows + t * n_exp, main_rows + (t + 1) * n_exp)
        for j in range(all_blocks):
            row_scr[rows, j * LANES : (j + 1) * LANES] = tail_scr[
                pl.ds(t * all_blocks + j, n_exp, stride=per_back), :
            ]
    if padded > total:
        row_scr[total:, :] = jnp.zeros((padded - total, width), F32)
    chunk = 2 * LANES
    for at in range(0, width, chunk):
        cols = slice(at, at + chunk)
        got = jnp.dot(left, row_scr[:, cols].astype(BF16), preferred_element_type=F32)
        out_ref[:, cols] = (
            got[:out_rows] + (got[out_rows : 2 * out_rows] + got[2 * out_rows :])
        ).astype(BF16)


def local(tokens, norm_gain, chosen_rows, route_weights, gate_weight, up_weight, down_weight):
    tok_rows, width = tokens.shape
    n_exp, slots = chosen_rows.shape
    half_slots = slots // 2
    n_main = half_slots // SUB * SUB
    n_tail = half_slots - n_main
    hidden = gate_weight.shape[2]
    chunk_rows = slots * (width // 2) // LANES
    block = jax.ShapeDtypeStruct((n_exp, chunk_rows, LANES), BF16)
    tails = n_exp * 2 * n_tail * (width // 2 // LANES)
    outgoing = pl.pallas_call(
        dispatch_kernel,
        out_shape=block,
        in_specs=[VMEM] * 3,
        out_specs=VMEM,
        scratch_shapes=[pltpu.VMEM((tok_rows, width // 2), BF16), pltpu.VMEM((tails, LANES), F32)],
        name="dispatch",
    )(tokens, norm_gain.reshape(1, width), chosen_rows)
    swap = [(0, 1), (1, 0)]
    mine = lax.all_to_all(outgoing, "ep", split_axis=0, concat_axis=0, tiled=True)
    other = lax.ppermute(mine, "tp", swap)
    rows = n_exp * slots
    send, keep = pl.pallas_call(
        functools.partial(expert_kernel, n_main=n_main, n_tail=n_tail),
        out_shape=[block, block],
        in_specs=[VMEM] * 5,
        out_specs=[VMEM, VMEM],
        scratch_shapes=[
            pltpu.VMEM((rows, width), BF16),
            pltpu.VMEM((rows, hidden), BF16),
            pltpu.VMEM((tails, LANES), F32),
            pltpu.VMEM((2, tails, LANES), F32),
        ],
        name="expert",
    )(mine, other, gate_weight, up_weight, down_weight)
    came = lax.ppermute(send, "tp", swap)
    summed = (keep.astype(F32) + came.astype(F32)).astype(BF16)
    back = lax.all_to_all(summed, "ep", split_axis=0, concat_axis=0, tiled=True)
    padded = cdiv(n_exp * half_slots, LANES) * LANES
    return pl.pallas_call(
        combine_kernel,
        out_shape=jax.ShapeDtypeStruct((tok_rows // 2, width), BF16),
        in_specs=[VMEM] * 3,
        out_specs=VMEM,
        scratch_shapes=[pltpu.VMEM((padded, width), F32), pltpu.VMEM((tails, LANES), F32)],
        name="combine",
    )(back, chosen_rows, route_weights)


def solution(mesh):
    return jax.shard_map(
        local,
        mesh=mesh,
        in_specs=(
            P(("grp", "ep"), None),
            P(),
            P("grp", "ep"),
            P("grp", "ep"),
            P("ep", None, "tp"),
            P("ep", None, "tp"),
            P("ep", "tp", None),
        ),
        out_specs=P(("grp", "ep", "tp"), None),
        check_vma=False,
    )
```

```python
import functools

import jax
import jax.numpy as jnp
from jax import lax
from jax.experimental import pallas as pl
from jax.experimental.pallas import tpu as pltpu
from jax.sharding import PartitionSpec as P

LANES = 128
SUB = 8
COPIES = 3
COVER_FLOPS = 4_000_000_000
VMEM_LIMIT = 32 * 1024 * 1024
F32 = jnp.float32
BF16 = jnp.bfloat16
VMEM = pl.BlockSpec(memory_space=pltpu.VMEM)
HBM = pl.BlockSpec(memory_space=pltpu.HBM)


def cdiv(a, b):
    return (a + b - 1) // b


def pick(values, wanted):
    lane = lax.broadcasted_iota(jnp.int32, values.shape, 1)
    return jnp.sum(jnp.where(lane == wanted, values, 0.0), axis=1, keepdims=True)


def main_slots(n_main, half_slots, slots):
    sub = lax.broadcasted_iota(jnp.int32, (2 * n_main, slots), 0)
    return jnp.where(sub < n_main, sub, sub - n_main + half_slots)


def dispatch_kernel(
    tok_hbm, gain_hbm, rows_hbm, weight_hbm, out_ref, rows_ref, weight_ref,
    tok_ref, gain_ref, norm_scr, tail_scr, sems,
):
    tok_rows, width = tok_ref.shape
    step = 16
    cuts = [tok_rows * k // COPIES // step * step for k in range(COPIES)] + [tok_rows]
    copies = [
        pltpu.make_async_copy(gain_hbm, gain_ref, sems.at[COPIES]),
        pltpu.make_async_copy(rows_hbm, rows_ref, sems.at[COPIES + 1]),
        pltpu.make_async_copy(weight_hbm, weight_ref, sems.at[COPIES + 2]),
    ]
    parts = [
        pltpu.make_async_copy(tok_hbm.at[low:high], tok_ref.at[low:high], sems.at[k])
        for k, (low, high) in enumerate(zip(cuts, cuts[1:]))
    ]
    for copy in copies + parts:
        copy.start()
    for copy in copies:
        copy.wait()
    n_dest, slots = rows_ref.shape
    half_slots = slots // 2
    n_main = half_slots // SUB * SUB
    n_tail = half_slots - n_main
    half_width = width // 2
    blocks = half_width // LANES
    core = lax.axis_index("tp")
    base = pl.multiple_of(core * half_width, half_width)
    half_blocks = half_width // LANES
    gains = gain_ref[...].astype(F32)
    gains = jnp.where(core == 0, gains[:half_blocks], gains[half_blocks:])
    gain = jnp.concatenate([gains[j : j + 1, :] for j in range(half_blocks)], axis=1)
    for at in range(0, tok_rows, step):
        if at in cuts:
            parts[cuts.index(at)].wait()
        rows = slice(at, at + step)
        values = tok_ref[rows, :].astype(F32)
        scale = lax.rsqrt(jnp.mean(values * values, axis=-1, keepdims=True) + 1e-06)
        part = tok_ref[rows, pl.ds(base, half_width)].astype(F32)
        norm_scr[rows, :] = (part * scale * gain).astype(BF16)
    normed = norm_scr[...]
    index = (rows_ref[...] - lax.axis_index("ep") * tok_rows).astype(F32)
    wanted = main_slots(n_main, half_slots, slots)
    group = 2 * n_main

    def one_hot(column):
        token = lax.broadcasted_iota(jnp.int32, (column.shape[0], tok_rows), 1)
        return jnp.where(token == column.astype(jnp.int32), 1.0, 0.0).astype(BF16)

    def chosen(column):
        return jnp.dot(one_hot(column), normed, preferred_element_type=F32)

    for first in range(0, n_dest, SUB):
        columns = [
            pick(jnp.broadcast_to(index[d : d + 1, :], (group, slots)), wanted)
            for d in range(first, first + SUB)
        ]
        got = chosen(jnp.concatenate(columns, axis=0))
        for d in range(SUB):
            for j in range(blocks):
                out_ref[first + d, j * group : (j + 1) * group, :] = got[
                    d * group : (d + 1) * group, j * LANES : (j + 1) * LANES
                ].astype(BF16)
    per_dest = 2 * n_tail * blocks
    columns = [
        pick(index, jnp.full((n_dest, slots), h * half_slots + n_main + t, jnp.int32))
        for h in range(2)
        for t in range(n_tail)
    ]
    got = chosen(jnp.concatenate(columns, axis=0))
    for k in range(2 * n_tail):
        for j in range(blocks):
            tail_scr[pl.ds(k * blocks + j, n_dest, stride=per_dest), :] = got[
                k * n_dest : (k + 1) * n_dest, j * LANES : (j + 1) * LANES
            ]
    for d in range(n_dest):
        out_ref[d, group * blocks :, :] = tail_scr[d * per_dest : (d + 1) * per_dest, :].astype(BF16)


def expert_kernel(
    mine_ref, other_ref, gate_ref, up_ref, down_ref, send_ref, keep_ref,
    x_scr, hidden_scr, tail_scr, back_scr, *, n_main, n_tail,
):
    n_src = mine_ref.shape[0]
    _, width, hidden = gate_ref.shape
    half_width = width // 2
    blocks = half_width // LANES
    group = 2 * n_main
    per_src = 2 * n_tail * blocks
    main_rows = n_src * group
    core = lax.axis_index("tp")
    for ref, base in ((mine_ref, core * half_width), (other_ref, (1 - core) * half_width)):
        for s in range(n_src):
            tail_scr[s * per_src : (s + 1) * per_src, :] = ref[s, group * blocks :, :].astype(F32)
        for j in range(blocks):
            lanes = pl.ds(pl.multiple_of(base + j * LANES, LANES), LANES)
            for s in range(n_src):
                x_scr[s * group : (s + 1) * group, lanes] = ref[s, j * group : (j + 1) * group, :]
            rest = [
                tail_scr[pl.ds(k * blocks + j, n_src, stride=per_src), :] for k in range(2 * n_tail)
            ]
            x_scr[main_rows:, lanes] = jnp.concatenate(rest, axis=0).astype(BF16)
    chunk = 2 * LANES
    x = x_scr[...]
    for at in range(0, hidden, chunk):
        cols = slice(at, at + chunk)
        gate = jnp.dot(x, gate_ref[0, :, cols], preferred_element_type=F32)
        up = jnp.dot(x, up_ref[0, :, cols], preferred_element_type=F32)
        hidden_scr[:, cols] = (gate / (1.0 + jnp.exp(-gate)) * up).astype(BF16)
    act = hidden_scr[...]
    first = core == 0
    all_blocks = width // LANES
    per_back = n_tail * all_blocks
    for at in range(0, width, chunk):
        part = jnp.dot(act, down_ref[0, :, at : at + chunk], preferred_element_type=F32)
        j = at // LANES
        for s in range(n_src):
            halves = []
            for h in range(2):
                row = s * group + h * n_main
                halves.append(
                    jnp.concatenate(
                        [part[row : row + n_main, :LANES], part[row : row + n_main, LANES:]], axis=0
                    )
                )
            place = slice(j * n_main, (j + 2) * n_main)
            send_ref[s, place, :] = jnp.where(first, halves[1], halves[0]).astype(BF16)
            keep_ref[s, place, :] = jnp.where(first, halves[0], halves[1]).astype(BF16)
        for b in range(2):
            lanes = slice(b * LANES, (b + 1) * LANES)
            for t in range(n_tail):
                rows = [main_rows + (h * n_tail + t) * n_src for h in range(2)]
                low, high = (part[row : row + n_src, lanes] for row in rows)
                where = pl.ds(t * all_blocks + j + b, n_src, stride=per_back)
                back_scr[0, where, :] = jnp.where(first, high, low)
                back_scr[1, where, :] = jnp.where(first, low, high)
    for s in range(n_src):
        rows = slice(s * per_back, (s + 1) * per_back)
        send_ref[s, n_main * all_blocks :, :] = back_scr[0, rows, :].astype(BF16)
        keep_ref[s, n_main * all_blocks :, :] = back_scr[1, rows, :].astype(BF16)


def route_kernel(rows_ref, weight_ref, left_ref):
    n_exp, slots = rows_ref.shape
    half_slots = slots // 2
    n_main = half_slots // SUB * SUB
    n_tail = half_slots - n_main
    out_rows = left_ref.shape[0] // 3
    core = lax.axis_index("tp")
    start = lax.axis_index("ep") * (2 * out_rows) + core * out_rows
    index = (rows_ref[...] - start).astype(F32)
    weight = weight_ref[...]
    lane0 = core * half_slots
    wanted = lax.broadcasted_iota(jnp.int32, (n_main, slots), 0) + lane0
    pieces = []

    def entry(idx, wgt):
        token = lax.broadcasted_iota(jnp.int32, (idx.shape[0], cdiv(out_rows, LANES) * LANES), 1)
        return jnp.where(token == idx.astype(jnp.int32), wgt, 0.0)

    for e in range(n_exp):
        columns = [
            pick(jnp.broadcast_to(v[e : e + 1, :], (n_main, slots)), wanted) for v in (index, weight)
        ]
        pieces.append(entry(*columns))
    for t in range(n_tail):
        at = jnp.full((n_exp, slots), n_main + t, jnp.int32) + lane0
        pieces.append(entry(pick(index, at), pick(weight, at)))
    total = n_exp * half_slots
    padded = cdiv(total, LANES) * LANES
    if padded > total:
        pieces.append(jnp.zeros((padded - total, pieces[0].shape[1]), F32))
    spread = jnp.concatenate(pieces, axis=0).T[:out_rows, :]
    high = spread.astype(BF16)
    rest = spread - high.astype(F32)
    mid = rest.astype(BF16)
    low = (rest - mid.astype(F32)).astype(BF16)
    left_ref[...] = jnp.concatenate([high, mid, low], axis=0)


def combine_kernel(back_ref, left_ref, out_ref, row_scr, tail_scr, *, n_main, n_tail):
    n_exp = back_ref.shape[0]
    out_rows, width = out_ref.shape
    all_blocks = width // LANES
    per_back = n_tail * all_blocks
    main_rows = n_exp * n_main
    total = n_exp * (n_main + n_tail)
    padded = row_scr.shape[0]
    left = left_ref[...]
    for e in range(n_exp):
        tail_scr[e * per_back : (e + 1) * per_back, :] = back_ref[e, n_main * all_blocks :, :].astype(F32)
        for j in range(0, all_blocks, 2):
            two = back_ref[e, j * n_main : (j + 2) * n_main, :].astype(F32)
            row_scr[e * n_main : (e + 1) * n_main, j * LANES : (j + 1) * LANES] = two[:n_main]
            row_scr[e * n_main : (e + 1) * n_main, (j + 1) * LANES : (j + 2) * LANES] = two[n_main:]
    for t in range(n_tail):
        rows = slice(main_rows + t * n_exp, main_rows + (t + 1) * n_exp)
        for j in range(all_blocks):
            row_scr[rows, j * LANES : (j + 1) * LANES] = tail_scr[
                pl.ds(t * all_blocks + j, n_exp, stride=per_back), :
            ]
    if padded > total:
        row_scr[total:, :] = jnp.zeros((padded - total, width), F32)
    chunk = 2 * LANES
    for at in range(0, width, chunk):
        cols = slice(at, at + chunk)
        got = jnp.dot(left, row_scr[:, cols].astype(BF16), preferred_element_type=F32)
        out_ref[:, cols] = (
            got[:out_rows] + (got[out_rows : 2 * out_rows] + got[2 * out_rows :])
        ).astype(BF16)


def local(tokens, norm_gain, chosen_rows, route_weights, gate_weight, up_weight, down_weight):
    tok_rows, width = tokens.shape
    n_exp, slots = chosen_rows.shape
    half_slots = slots // 2
    n_main = half_slots // SUB * SUB
    n_tail = half_slots - n_main
    hidden = gate_weight.shape[2]
    chunk_rows = slots * (width // 2) // LANES
    block = jax.ShapeDtypeStruct((n_exp, chunk_rows, LANES), BF16)
    tails = n_exp * 2 * n_tail * (width // 2 // LANES)
    args = (tokens, norm_gain.reshape(width // LANES, LANES), chosen_rows, route_weights)
    outgoing, own_rows, own_weights = pl.pallas_call(
        dispatch_kernel,
        out_shape=[block] + [jax.ShapeDtypeStruct(x.shape, x.dtype) for x in (chosen_rows, route_weights)],
        in_specs=[HBM] * 4,
        out_specs=[VMEM] * 3,
        scratch_shapes=[
            pltpu.VMEM((tok_rows, width), BF16),
            pltpu.VMEM((width // LANES, LANES), BF16),
            pltpu.VMEM((tok_rows, width // 2), BF16),
            pltpu.VMEM((tails, LANES), F32),
            pltpu.SemaphoreType.DMA((COPIES + 3,)),
        ],
        compiler_params=pltpu.CompilerParams(vmem_limit_bytes=VMEM_LIMIT),
        name="dispatch",
    )(*(pltpu.with_memory_space_constraint(x, pltpu.HBM) for x in args))
    left_shape = (3 * (tok_rows // 2), cdiv(n_exp * half_slots, LANES) * LANES)
    weight_bytes = 3 * 2 * width * hidden
    left = pl.pallas_call(
        route_kernel,
        out_shape=jax.ShapeDtypeStruct(left_shape, BF16),
        in_specs=[VMEM] * 2,
        out_specs=VMEM,
        compiler_params=pltpu.CompilerParams(vmem_limit_bytes=VMEM_LIMIT),
        cost_estimate=pl.CostEstimate(
            flops=COVER_FLOPS, bytes_accessed=weight_bytes, transcendentals=0
        ),
        name="route",
    )(own_rows, own_weights)
    outgoing, left = lax.optimization_barrier((outgoing, left))
    swap = [(0, 1), (1, 0)]
    mine = lax.all_to_all(outgoing, "ep", split_axis=0, concat_axis=0, tiled=True)
    other = lax.ppermute(mine, "tp", swap)
    rows = n_exp * slots
    send, keep = pl.pallas_call(
        functools.partial(expert_kernel, n_main=n_main, n_tail=n_tail),
        out_shape=[block, block],
        in_specs=[VMEM] * 5,
        out_specs=[VMEM, VMEM],
        scratch_shapes=[
            pltpu.VMEM((rows, width), BF16),
            pltpu.VMEM((rows, hidden), BF16),
            pltpu.VMEM((tails, LANES), F32),
            pltpu.VMEM((2, tails, LANES), F32),
        ],
        compiler_params=pltpu.CompilerParams(vmem_limit_bytes=VMEM_LIMIT),
        name="expert",
    )(mine, other, gate_weight, up_weight, down_weight)
    came = lax.ppermute(send, "tp", swap)
    summed = (keep.astype(F32) + came.astype(F32)).astype(BF16)
    back = lax.all_to_all(summed, "ep", split_axis=0, concat_axis=0, tiled=True)
    return pl.pallas_call(
        functools.partial(combine_kernel, n_main=n_main, n_tail=n_tail),
        out_shape=jax.ShapeDtypeStruct((tok_rows // 2, width), BF16),
        in_specs=[VMEM] * 2,
        out_specs=VMEM,
        scratch_shapes=[pltpu.VMEM((left_shape[1], width), F32), pltpu.VMEM((tails, LANES), F32)],
        compiler_params=pltpu.CompilerParams(vmem_limit_bytes=VMEM_LIMIT),
        name="combine",
    )(back, left)


def solution(mesh):
    return jax.shard_map(
        local,
        mesh=mesh,
        in_specs=(
            P(("grp", "ep"), None),
            P(),
            P("grp", "ep"),
            P("grp", "ep"),
            P("ep", None, "tp"),
            P("ep", None, "tp"),
            P("ep", "tp", None),
        ),
        out_specs=P(("grp", "ep", "tp"), None),
        check_vma=False,
    )
```

```python
import functools

import jax
import jax.numpy as jnp
from jax import lax
from jax.experimental import pallas as pl
from jax.experimental.pallas import tpu as pltpu
from jax.sharding import PartitionSpec as P

LANES = 128
SUB = 8
COPIES = 3
COVER_FLOPS = 4_000_000_000
VMEM_LIMIT = 32 * 1024 * 1024
F32 = jnp.float32
BF16 = jnp.bfloat16
SWAP = [(0, 1), (1, 0)]
VMEM = pl.BlockSpec(memory_space=pltpu.VMEM)
HBM = pl.BlockSpec(memory_space=pltpu.HBM)


def cdiv(a, b):
    return (a + b - 1) // b


def partner(core, m, count):
    return lax.axis_index("ep") ^ (2 * (count - 1 - m) + core)


def pick(values, wanted):
    lane = lax.broadcasted_iota(jnp.int32, values.shape, 1)
    return jnp.sum(jnp.where(lane == wanted, values, 0.0), axis=1, keepdims=True)


def split_slots(slots):
    half_slots = slots // 2
    n_main = half_slots // SUB * SUB
    return half_slots, n_main, half_slots - n_main


def dispatch_kernel(*refs, count):
    tok_hbm, gain_hbm, rows_hbm, weight_hbm = refs[:4]
    outs = refs[4 : 4 + count]
    rows_ref, weight_ref, tok_ref, gain_ref, norm_scr, tail_scr, index_scr, sems = refs[4 + count :]
    tok_rows, width = tok_ref.shape
    slots = rows_ref.shape[1]
    step = 16
    cuts = [tok_rows * k // COPIES // step * step for k in range(COPIES)] + [tok_rows]
    copies = [
        pltpu.make_async_copy(gain_hbm, gain_ref, sems.at[COPIES]),
        pltpu.make_async_copy(rows_hbm, rows_ref, sems.at[COPIES + 1]),
        pltpu.make_async_copy(weight_hbm, weight_ref, sems.at[COPIES + 2]),
    ]
    parts = [
        pltpu.make_async_copy(tok_hbm.at[low:high], tok_ref.at[low:high], sems.at[k])
        for k, (low, high) in enumerate(zip(cuts, cuts[1:]))
    ]
    for copy in copies + parts:
        copy.start()
    for copy in copies:
        copy.wait()
    half_slots, n_main, n_tail = split_slots(slots)
    group = 2 * n_main
    blocks = width // LANES
    core = lax.axis_index("tp")
    index_scr[...] = jnp.zeros_like(index_scr)
    for m in range(count):
        index_scr[m : m + 1, :] = rows_ref[pl.ds(partner(core, m, count), 1), :]
    index = (index_scr[...] - lax.axis_index("ep") * tok_rows).astype(F32)
    sub = lax.broadcasted_iota(jnp.int32, (group, slots), 0)
    wanted = jnp.where(sub < n_main, sub, sub - n_main + half_slots)

    def one_hot(column):
        token = lax.broadcasted_iota(jnp.int32, (column.shape[0], tok_rows), 1)
        return jnp.where(token == column.astype(jnp.int32), 1.0, 0.0).astype(BF16)

    mains = [
        one_hot(pick(jnp.broadcast_to(index[m : m + 1, :], (group, slots)), wanted))
        for m in range(count)
    ]
    tails = [
        one_hot(pick(index, jnp.full(index.shape, h * half_slots + n_main + t, jnp.int32)))
        for h in range(2)
        for t in range(n_tail)
    ]
    gains = gain_ref[...].astype(F32)
    gain = jnp.concatenate([gains[j : j + 1, :] for j in range(blocks)], axis=1)
    for at in range(0, tok_rows, step):
        if at in cuts:
            parts[cuts.index(at)].wait()
        rows = slice(at, at + step)
        values = tok_ref[rows, :].astype(F32)
        scale = lax.rsqrt(jnp.mean(values * values, axis=-1, keepdims=True) + 1e-06)
        norm_scr[rows, :] = (values * scale * gain).astype(BF16)
    normed = norm_scr[...]
    together = 8
    for first in range(0, count, together):
        members = range(first, min(first + together, count))
        got = jnp.dot(
            jnp.concatenate([mains[m] for m in members], axis=0), normed, preferred_element_type=F32
        )
        for m in members:
            at = (m - first) * group
            for j in range(blocks):
                outs[m][j * group : (j + 1) * group, :] = got[
                    at : at + group, j * LANES : (j + 1) * LANES
                ].astype(BF16)
    got = jnp.dot(jnp.concatenate(tails, axis=0), normed, preferred_element_type=F32)
    padded = index.shape[0]
    per_block = 2 * n_tail * blocks
    for k in range(2 * n_tail):
        for j in range(blocks):
            tail_scr[pl.ds(k * blocks + j, padded, stride=per_block), :] = got[
                k * padded : (k + 1) * padded, j * LANES : (j + 1) * LANES
            ]
    for m in range(count):
        outs[m][group * blocks :, :] = tail_scr[m * per_block : (m + 1) * per_block, :].astype(BF16)


def expert_kernel(*refs, count, slots):
    mine, other = refs[:count], refs[count : 2 * count]
    gate_ref, up_ref, down_ref = refs[2 * count : 2 * count + 3]
    send, keep = refs[2 * count + 3 : 3 * count + 3], refs[3 * count + 3 : 4 * count + 3]
    x_scr, hidden_scr, tail_scr, back_scr = refs[4 * count + 3 :]
    _, width, hidden = gate_ref.shape
    n_main, n_tail = split_slots(slots)[1:]
    group = 2 * n_main
    blocks = width // LANES
    n_src = 2 * count
    main_rows = n_src * group
    per_block = 2 * n_tail * blocks
    core = lax.axis_index("tp")
    for side, base in ((mine, core * count), (other, (1 - core) * count)):
        for m in range(count):
            rows = pl.ds(pl.multiple_of((base + m) * group, group), group)
            for j in range(blocks):
                x_scr[rows, j * LANES : (j + 1) * LANES] = side[m][j * group : (j + 1) * group, :]
            rows = pl.ds(pl.multiple_of((base + m) * per_block, per_block), per_block)
            tail_scr[rows, :] = side[m][group * blocks :, :].astype(F32)
    for j in range(blocks):
        rest = [
            tail_scr[pl.ds(k * blocks + j, n_src, stride=per_block), :] for k in range(2 * n_tail)
        ]
        x_scr[main_rows:, j * LANES : (j + 1) * LANES] = jnp.concatenate(rest, axis=0).astype(BF16)
    chunk = 2 * LANES
    x = x_scr[...]
    for at in range(0, hidden, chunk):
        cols = slice(at, at + chunk)
        gate = jnp.dot(x, gate_ref[0, :, cols], preferred_element_type=F32)
        up = jnp.dot(x, up_ref[0, :, cols], preferred_element_type=F32)
        hidden_scr[:, cols] = (gate / (1.0 + jnp.exp(-gate)) * up).astype(BF16)
    act = hidden_scr[...]
    first = core == 0
    for at in range(0, width, chunk):
        part = jnp.dot(act, down_ref[0, :, at : at + chunk], preferred_element_type=F32)
        for b in range(chunk // LANES):
            lanes = slice(b * LANES, (b + 1) * LANES)
            j = at // LANES + b
            place = slice(j * group, (j + 1) * group)
            for m in range(count):
                low, high = (part[(s + m) * group : (s + m + 1) * group, lanes] for s in (0, count))
                send[m][place, :] = jnp.where(first, high, low).astype(BF16)
                keep[m][place, :] = jnp.where(first, low, high).astype(BF16)
            for k in range(2 * n_tail):
                row = main_rows + k * n_src
                back_scr[pl.ds(k * blocks + j, n_src, stride=per_block), :] = part[row : row + n_src, lanes]
    for m in range(count):
        low, high = (back_scr[(s + m) * per_block : (s + m + 1) * per_block, :] for s in (0, count))
        send[m][group * blocks :, :] = jnp.where(first, high, low).astype(BF16)
        keep[m][group * blocks :, :] = jnp.where(first, low, high).astype(BF16)


def route_kernel(rows_ref, weight_ref, left_ref, index_scr, weight_scr):
    n_exp, slots = rows_ref.shape
    half_slots, n_main, n_tail = split_slots(slots)
    count = n_exp // 2
    out_rows = left_ref.shape[0] // 3
    core = lax.axis_index("tp")
    for side in range(2):
        for m in range(count):
            b = side * count + m
            row = pl.ds(partner(side, m, count), 1)
            index_scr[b : b + 1, :] = rows_ref[row, :]
            weight_scr[b : b + 1, :] = weight_ref[row, :]
    start = lax.axis_index("ep") * (2 * out_rows) + core * out_rows
    index = (index_scr[...] - start).astype(F32)
    weight = weight_scr[...]
    lane0 = core * half_slots
    wanted = lax.broadcasted_iota(jnp.int32, (n_main, slots), 0) + lane0
    pieces = []

    def entry(idx, wgt):
        token = lax.broadcasted_iota(jnp.int32, (idx.shape[0], cdiv(out_rows, LANES) * LANES), 1)
        return jnp.where(token == idx.astype(jnp.int32), wgt, 0.0)

    for e in range(n_exp):
        columns = [
            pick(jnp.broadcast_to(v[e : e + 1, :], (n_main, slots)), wanted) for v in (index, weight)
        ]
        pieces.append(entry(*columns))
    for t in range(n_tail):
        at = jnp.full((n_exp, slots), n_main + t, jnp.int32) + lane0
        pieces.append(entry(pick(index, at), pick(weight, at)))
    total = n_exp * half_slots
    padded = left_ref.shape[1]
    if padded > total:
        pieces.append(jnp.zeros((padded - total, pieces[0].shape[1]), F32))
    spread = jnp.concatenate(pieces, axis=0).T[:out_rows, :]
    high = spread.astype(BF16)
    rest = spread - high.astype(F32)
    mid = rest.astype(BF16)
    low = (rest - mid.astype(F32)).astype(BF16)
    left_ref[...] = jnp.concatenate([high, mid, low], axis=0)


def combine_kernel(*refs, count, slots):
    mine, other = refs[:count], refs[count : 2 * count]
    left_ref, out_ref, row_scr, tail_scr = refs[2 * count :]
    n_exp = 2 * count
    out_rows, width = out_ref.shape
    half_slots, n_main, n_tail = split_slots(slots)
    group = 2 * n_main
    blocks = width // LANES
    per_half = n_tail * blocks
    main_rows = n_exp * n_main
    total = n_exp * half_slots
    padded = row_scr.shape[0]
    core = lax.axis_index("tp")
    first = core == 0
    for side, base in ((mine, core * count), (other, (1 - core) * count)):
        for m in range(count):
            rows = pl.ds(pl.multiple_of((base + m) * n_main, n_main), n_main)
            for j in range(blocks):
                two = side[m][j * group : (j + 1) * group, :].astype(F32)
                row_scr[rows, j * LANES : (j + 1) * LANES] = jnp.where(first, two[:n_main], two[n_main:])
            two = side[m][group * blocks :, :].astype(F32)
            rows = pl.ds(pl.multiple_of((base + m) * per_half, per_half), per_half)
            tail_scr[rows, :] = jnp.where(first, two[:per_half], two[per_half:])
    for t in range(n_tail):
        rows = slice(main_rows + t * n_exp, main_rows + (t + 1) * n_exp)
        for j in range(blocks):
            row_scr[rows, j * LANES : (j + 1) * LANES] = tail_scr[
                pl.ds(t * blocks + j, n_exp, stride=per_half), :
            ]
    if padded > total:
        row_scr[total:, :] = jnp.zeros((padded - total, width), F32)
    left = left_ref[...]
    chunk = 2 * LANES
    for at in range(0, width, chunk):
        cols = slice(at, at + chunk)
        got = jnp.dot(left, row_scr[:, cols].astype(BF16), preferred_element_type=F32)
        out_ref[:, cols] = (
            got[:out_rows] + (got[out_rows : 2 * out_rows] + got[2 * out_rows :])
        ).astype(BF16)


def exchange(blocks, n_exp):
    count = len(blocks)
    came = []
    for m, block in enumerate(blocks):
        far = 2 * (count - 1 - m)
        pairs = [(2 * e + c, 2 * (e ^ (far + c)) + c) for e in range(n_exp) for c in range(2)]
        came.append(lax.ppermute(block, ("ep", "tp"), pairs))
    return came + [lax.ppermute(block, "tp", SWAP) for block in came]


def local(tokens, norm_gain, chosen_rows, route_weights, gate_weight, up_weight, down_weight):
    tok_rows, width = tokens.shape
    n_exp, slots = chosen_rows.shape
    half_slots, n_main, n_tail = split_slots(slots)
    count = n_exp // 2
    hidden = gate_weight.shape[2]
    blocks = width // LANES
    block = jax.ShapeDtypeStruct((slots * blocks, LANES), BF16)
    padded = cdiv(count, SUB) * SUB
    args = (tokens, norm_gain.reshape(blocks, LANES), chosen_rows, route_weights)
    params = pltpu.CompilerParams(vmem_limit_bytes=VMEM_LIMIT)
    *outgoing, own_rows, own_weights = pl.pallas_call(
        functools.partial(dispatch_kernel, count=count),
        out_shape=[block] * count
        + [jax.ShapeDtypeStruct(x.shape, x.dtype) for x in (chosen_rows, route_weights)],
        in_specs=[HBM] * 4,
        out_specs=[VMEM] * (count + 2),
        scratch_shapes=[
            pltpu.VMEM((tok_rows, width), BF16),
            pltpu.VMEM((blocks, LANES), BF16),
            pltpu.VMEM((tok_rows, width), BF16),
            pltpu.VMEM((padded * 2 * n_tail * blocks, LANES), F32),
            pltpu.VMEM((padded, slots), jnp.int32),
            pltpu.SemaphoreType.DMA((COPIES + 3,)),
        ],
        compiler_params=params,
        name="dispatch",
    )(*(pltpu.with_memory_space_constraint(x, pltpu.HBM) for x in args))
    left_shape = (3 * (tok_rows // 2), cdiv(n_exp * half_slots, LANES) * LANES)
    weight_bytes = 3 * 2 * width * hidden
    left = pl.pallas_call(
        route_kernel,
        out_shape=jax.ShapeDtypeStruct(left_shape, BF16),
        in_specs=[VMEM] * 2,
        out_specs=VMEM,
        scratch_shapes=[pltpu.VMEM((n_exp, slots), jnp.int32), pltpu.VMEM((n_exp, slots), F32)],
        compiler_params=params,
        cost_estimate=pl.CostEstimate(
            flops=COVER_FLOPS, bytes_accessed=weight_bytes, transcendentals=0
        ),
        name="route",
    )(own_rows, own_weights)
    *outgoing, left = lax.optimization_barrier((*outgoing, left))
    arrived = exchange(outgoing, n_exp)
    tails = n_exp * 2 * n_tail * blocks
    results = pl.pallas_call(
        functools.partial(expert_kernel, count=count, slots=slots),
        out_shape=[block] * (2 * count),
        in_specs=[VMEM] * (2 * count + 3),
        out_specs=[VMEM] * (2 * count),
        scratch_shapes=[
            pltpu.VMEM((n_exp * slots, width), BF16),
            pltpu.VMEM((n_exp * slots, hidden), BF16),
            pltpu.VMEM((tails, LANES), F32),
            pltpu.VMEM((tails, LANES), F32),
        ],
        compiler_params=params,
        name="expert",
    )(*arrived, gate_weight, up_weight, down_weight)
    came = [lax.ppermute(part, "tp", SWAP) for part in results[:count]]
    summed = [(a.astype(F32) + b.astype(F32)).astype(BF16) for a, b in zip(results[count:], came)]
    back = exchange(summed, n_exp)
    return pl.pallas_call(
        functools.partial(combine_kernel, count=count, slots=slots),
        out_shape=jax.ShapeDtypeStruct((tok_rows // 2, width), BF16),
        in_specs=[VMEM] * (2 * count + 1),
        out_specs=VMEM,
        scratch_shapes=[
            pltpu.VMEM((left_shape[1], width), F32),
            pltpu.VMEM((n_exp * n_tail * blocks, LANES), F32),
        ],
        compiler_params=params,
        name="combine",
    )(*back, left)


def solution(mesh):
    return jax.shard_map(
        local,
        mesh=mesh,
        in_specs=(
            P(("grp", "ep"), None),
            P(),
            P("grp", "ep"),
            P("grp", "ep"),
            P("ep", None, "tp"),
            P("ep", None, "tp"),
            P("ep", "tp", None),
        ),
        out_specs=P(("grp", "ep", "tp"), None),
        check_vma=False,
    )
```

```python
import functools

import jax
import jax.numpy as jnp
from jax import lax
from jax.experimental import pallas as pl
from jax.experimental.pallas import tpu as pltpu
from jax.sharding import PartitionSpec as P


LANES = 128
SUB = 8
COPIES = 3
TOGETHER = 1
COVER_FLOPS = 4_000_000_000
VMEM_LIMIT = 32 * 1024 * 1024
F32 = jnp.float32
BF16 = jnp.bfloat16
SWAP = [(0, 1), (1, 0)]
VMEM = pl.BlockSpec(memory_space=pltpu.VMEM)
HBM = pl.BlockSpec(memory_space=pltpu.HBM)


def cdiv(a, b):
    return (a + b - 1) // b


def turn(core, m):
    return 1 - core if m == 0 else core


def partner(core, m, count):
    return lax.axis_index("ep") ^ (2 * (count - 1 - m) + turn(core, m))


def pick(values, wanted):
    lane = lax.broadcasted_iota(jnp.int32, values.shape, 1)
    return jnp.sum(jnp.where(lane == wanted, values, 0.0), axis=1, keepdims=True)


def split_slots(slots):
    half_slots = slots // 2
    n_main = half_slots // SUB * SUB
    return half_slots, n_main, half_slots - n_main


def dispatch_kernel(*refs, count):
    tok_hbm, gain_hbm, rows_hbm, weight_hbm = refs[:4]
    outs = refs[4 : 4 + count]
    rows_ref, weight_ref, tok_ref, gain_ref, norm_scr, tail_scr, index_scr, sems = refs[4 + count :]
    tok_rows, width = tok_ref.shape
    slots = rows_ref.shape[1]
    step = 16
    cuts = [tok_rows * k // COPIES // step * step for k in range(COPIES)] + [tok_rows]
    copies = [
        pltpu.make_async_copy(gain_hbm, gain_ref, sems.at[COPIES]),
        pltpu.make_async_copy(rows_hbm, rows_ref, sems.at[COPIES + 1]),
        pltpu.make_async_copy(weight_hbm, weight_ref, sems.at[COPIES + 2]),
    ]
    parts = [
        pltpu.make_async_copy(tok_hbm.at[low:high], tok_ref.at[low:high], sems.at[k])
        for k, (low, high) in enumerate(zip(cuts, cuts[1:]))
    ]
    for copy in copies + parts:
        copy.start()
    for copy in copies:
        copy.wait()
    half_slots, n_main, n_tail = split_slots(slots)
    group = 2 * n_main
    blocks = width // LANES
    core = lax.axis_index("tp")
    index_scr[...] = jnp.zeros_like(index_scr)
    for m in range(count):
        index_scr[m : m + 1, :] = rows_ref[pl.ds(partner(core, m, count), 1), :]
    index = (index_scr[...] - lax.axis_index("ep") * tok_rows).astype(F32)
    sub = lax.broadcasted_iota(jnp.int32, (group, slots), 0)
    wanted = jnp.where(sub < n_main, sub, sub - n_main + half_slots)

    def one_hot(column):
        token = lax.broadcasted_iota(jnp.int32, (column.shape[0], tok_rows), 1)
        return jnp.where(token == column.astype(jnp.int32), 1.0, 0.0).astype(BF16)

    mains = [
        one_hot(pick(jnp.broadcast_to(index[m : m + 1, :], (group, slots)), wanted))
        for m in range(count)
    ]
    tails = [
        one_hot(pick(index, jnp.full(index.shape, h * half_slots + n_main + t, jnp.int32)))
        for h in range(2)
        for t in range(n_tail)
    ]
    gains = gain_ref[...].astype(F32)
    gain = jnp.concatenate([gains[j : j + 1, :] for j in range(blocks)], axis=1)
    for at in range(0, tok_rows, step):
        if at in cuts:
            parts[cuts.index(at)].wait()
        rows = slice(at, at + step)
        values = tok_ref[rows, :].astype(F32)
        scale = lax.rsqrt(jnp.mean(values * values, axis=-1, keepdims=True) + 1e-06)
        norm_scr[rows, :] = (values * scale * gain).astype(BF16)
    normed = norm_scr[...]
    together = 8
    for first in range(0, count, together):
        members = range(first, min(first + together, count))
        got = jnp.dot(
            jnp.concatenate([mains[m] for m in members], axis=0), normed, preferred_element_type=F32
        )
        for m in members:
            at = (m - first) * group
            for j in range(blocks):
                outs[m][j * group : (j + 1) * group, :] = got[
                    at : at + group, j * LANES : (j + 1) * LANES
                ].astype(BF16)
    got = jnp.dot(jnp.concatenate(tails, axis=0), normed, preferred_element_type=F32)
    padded = index.shape[0]
    per_block = 2 * n_tail * blocks
    for k in range(2 * n_tail):
        for j in range(blocks):
            tail_scr[pl.ds(k * blocks + j, padded, stride=per_block), :] = got[
                k * padded : (k + 1) * padded, j * LANES : (j + 1) * LANES
            ]
    for m in range(count):
        outs[m][group * blocks :, :] = tail_scr[m * per_block : (m + 1) * per_block, :].astype(BF16)


def expert_kernel(*refs, count, slots):
    mine, other = refs[:count], refs[count : 2 * count]
    gate_ref, up_ref, down_ref = refs[2 * count : 2 * count + 3]
    sends = count // TOGETHER
    rest = refs[2 * count + 3 :]
    rows = slots * gate_ref.shape[1] // LANES
    send = [rest[m // TOGETHER].at[pl.ds(m % TOGETHER * rows, rows)] for m in range(count)]
    keep = rest[sends : sends + count]
    x_scr, hidden_scr, tail_scr, back_scr = rest[sends + count :]
    _, width, hidden = gate_ref.shape
    n_main, n_tail = split_slots(slots)[1:]
    group = 2 * n_main
    blocks = width // LANES
    n_src = 2 * count
    main_rows = n_src * group
    per_block = 2 * n_tail * blocks
    core = lax.axis_index("tp")
    for side, base in ((mine, core * count), (other, (1 - core) * count)):
        for m in range(count):
            rows = pl.ds(pl.multiple_of((base + m) * group, group), group)
            for j in range(blocks):
                x_scr[rows, j * LANES : (j + 1) * LANES] = side[m][j * group : (j + 1) * group, :]
            rows = pl.ds(pl.multiple_of((base + m) * per_block, per_block), per_block)
            tail_scr[rows, :] = side[m][group * blocks :, :].astype(F32)
    for j in range(blocks):
        rest = [
            tail_scr[pl.ds(k * blocks + j, n_src, stride=per_block), :] for k in range(2 * n_tail)
        ]
        x_scr[main_rows:, j * LANES : (j + 1) * LANES] = jnp.concatenate(rest, axis=0).astype(BF16)
    chunk = 2 * LANES
    x = x_scr[...]
    for at in range(0, hidden, chunk):
        cols = slice(at, at + chunk)
        gate = jnp.dot(x, gate_ref[0, :, cols], preferred_element_type=F32)
        up = jnp.dot(x, up_ref[0, :, cols], preferred_element_type=F32)
        hidden_scr[:, cols] = (gate / (1.0 + jnp.exp(-gate)) * up).astype(BF16)
    act = hidden_scr[...]
    first = core == 0
    for at in range(0, width, chunk):
        part = jnp.dot(act, down_ref[0, :, at : at + chunk], preferred_element_type=F32)
        for b in range(chunk // LANES):
            lanes = slice(b * LANES, (b + 1) * LANES)
            j = at // LANES + b
            place = slice(j * group, (j + 1) * group)
            for m in range(count):
                low, high = (part[(s + m) * group : (s + m + 1) * group, lanes] for s in (0, count))
                send[m][place, :] = jnp.where(first, high, low).astype(BF16)
                keep[m][place, :] = jnp.where(first, low, high).astype(BF16)
            for k in range(2 * n_tail):
                row = main_rows + k * n_src
                back_scr[pl.ds(k * blocks + j, n_src, stride=per_block), :] = part[row : row + n_src, lanes]
    for m in range(count):
        low, high = (back_scr[(s + m) * per_block : (s + m + 1) * per_block, :] for s in (0, count))
        send[m][group * blocks :, :] = jnp.where(first, high, low).astype(BF16)
        keep[m][group * blocks :, :] = jnp.where(first, low, high).astype(BF16)


def route_kernel(rows_ref, weight_ref, left_ref, index_scr, weight_scr):
    n_exp, slots = rows_ref.shape
    half_slots, n_main, n_tail = split_slots(slots)
    count = n_exp // 2
    out_rows = left_ref.shape[0] // 3
    core = lax.axis_index("tp")
    for side in range(2):
        for m in range(count):
            b = side * count + m
            row = pl.ds(partner(side, m, count), 1)
            index_scr[b : b + 1, :] = rows_ref[row, :]
            weight_scr[b : b + 1, :] = weight_ref[row, :]
    start = lax.axis_index("ep") * (2 * out_rows) + core * out_rows
    index = (index_scr[...] - start).astype(F32)
    weight = weight_scr[...]
    lane0 = core * half_slots
    wanted = lax.broadcasted_iota(jnp.int32, (n_main, slots), 0) + lane0
    pieces = []

    def entry(idx, wgt):
        token = lax.broadcasted_iota(jnp.int32, (idx.shape[0], cdiv(out_rows, LANES) * LANES), 1)
        return jnp.where(token == idx.astype(jnp.int32), wgt, 0.0)

    for e in range(n_exp):
        columns = [
            pick(jnp.broadcast_to(v[e : e + 1, :], (n_main, slots)), wanted) for v in (index, weight)
        ]
        pieces.append(entry(*columns))
    for t in range(n_tail):
        at = jnp.full((n_exp, slots), n_main + t, jnp.int32) + lane0
        pieces.append(entry(pick(index, at), pick(weight, at)))
    total = n_exp * half_slots
    padded = left_ref.shape[1]
    if padded > total:
        pieces.append(jnp.zeros((padded - total, pieces[0].shape[1]), F32))
    spread = jnp.concatenate(pieces, axis=0).T[:out_rows, :]
    high = spread.astype(BF16)
    rest = spread - high.astype(F32)
    mid = rest.astype(BF16)
    low = (rest - mid.astype(F32)).astype(BF16)
    left_ref[...] = jnp.concatenate([high, mid, low], axis=0)


def combine_kernel(*refs, count, slots):
    mine, other = refs[:count], refs[count : 2 * count]
    left_ref, out_ref, row_scr, tail_scr = refs[2 * count :]
    n_exp = 2 * count
    out_rows, width = out_ref.shape
    half_slots, n_main, n_tail = split_slots(slots)
    group = 2 * n_main
    blocks = width // LANES
    per_half = n_tail * blocks
    main_rows = n_exp * n_main
    total = n_exp * half_slots
    padded = row_scr.shape[0]
    core = lax.axis_index("tp")
    first = core == 0
    for side, base in ((mine, core * count), (other, (1 - core) * count)):
        for m in range(count):
            rows = pl.ds(pl.multiple_of((base + m) * n_main, n_main), n_main)
            for j in range(blocks):
                two = side[m][j * group : (j + 1) * group, :].astype(F32)
                row_scr[rows, j * LANES : (j + 1) * LANES] = jnp.where(first, two[:n_main], two[n_main:])
            two = side[m][group * blocks :, :].astype(F32)
            rows = pl.ds(pl.multiple_of((base + m) * per_half, per_half), per_half)
            tail_scr[rows, :] = jnp.where(first, two[:per_half], two[per_half:])
    for t in range(n_tail):
        rows = slice(main_rows + t * n_exp, main_rows + (t + 1) * n_exp)
        for j in range(blocks):
            row_scr[rows, j * LANES : (j + 1) * LANES] = tail_scr[
                pl.ds(t * blocks + j, n_exp, stride=per_half), :
            ]
    if padded > total:
        row_scr[total:, :] = jnp.zeros((padded - total, width), F32)
    left = left_ref[...]
    chunk = 2 * LANES
    for at in range(0, width, chunk):
        cols = slice(at, at + chunk)
        got = jnp.dot(left, row_scr[:, cols].astype(BF16), preferred_element_type=F32)
        out_ref[:, cols] = (
            got[:out_rows] + (got[out_rows : 2 * out_rows] + got[2 * out_rows :])
        ).astype(BF16)


def exchange(blocks, n_exp):
    count = len(blocks)
    came, passed = [], []
    for m, block in enumerate(blocks):
        far = 2 * (count - 1 - m)
        pairs = [(2 * e + c, 2 * (e ^ (far + turn(c, m))) + c) for e in range(n_exp) for c in range(2)]
        came.append(lax.ppermute(block, ("ep", "tp"), pairs))
    for block in came:
        passed.append(lax.ppermute(block, "tp", SWAP))
    return came + passed


def local(tokens, norm_gain, chosen_rows, route_weights, gate_weight, up_weight, down_weight):
    tok_rows, width = tokens.shape
    n_exp, slots = chosen_rows.shape
    half_slots, _, n_tail = split_slots(slots)
    count = n_exp // 2
    hidden = gate_weight.shape[2]
    blocks = width // LANES
    block = jax.ShapeDtypeStruct((slots * blocks, LANES), BF16)
    several = jax.ShapeDtypeStruct((TOGETHER * slots * blocks, LANES), BF16)
    padded = cdiv(count, SUB) * SUB
    args = (tokens, norm_gain.reshape(blocks, LANES), chosen_rows, route_weights)
    params = pltpu.CompilerParams(vmem_limit_bytes=VMEM_LIMIT)
    *outgoing, own_rows, own_weights = pl.pallas_call(
        functools.partial(dispatch_kernel, count=count),
        out_shape=[block] * count
        + [jax.ShapeDtypeStruct(x.shape, x.dtype) for x in (chosen_rows, route_weights)],
        in_specs=[HBM] * 4,
        out_specs=[VMEM] * (count + 2),
        scratch_shapes=[
            pltpu.VMEM((tok_rows, width), BF16),
            pltpu.VMEM((blocks, LANES), BF16),
            pltpu.VMEM((tok_rows, width), BF16),
            pltpu.VMEM((padded * 2 * n_tail * blocks, LANES), F32),
            pltpu.VMEM((padded, slots), jnp.int32),
            pltpu.SemaphoreType.DMA((COPIES + 3,)),
        ],
        compiler_params=params,
        name="dispatch",
    )(*(pltpu.with_memory_space_constraint(x, pltpu.HBM) for x in args))
    left_shape = (3 * (tok_rows // 2), cdiv(n_exp * half_slots, LANES) * LANES)
    weight_bytes = 3 * 2 * width * hidden
    left = pl.pallas_call(
        route_kernel,
        out_shape=jax.ShapeDtypeStruct(left_shape, BF16),
        in_specs=[VMEM] * 2,
        out_specs=VMEM,
        scratch_shapes=[pltpu.VMEM((n_exp, slots), jnp.int32), pltpu.VMEM((n_exp, slots), F32)],
        compiler_params=params,
        cost_estimate=pl.CostEstimate(
            flops=COVER_FLOPS, bytes_accessed=weight_bytes, transcendentals=0
        ),
        name="route",
    )(own_rows, own_weights)
    arrived = exchange(outgoing, n_exp)
    tails = n_exp * 2 * n_tail * blocks
    results = pl.pallas_call(
        functools.partial(expert_kernel, count=count, slots=slots),
        out_shape=[several] * (count // TOGETHER) + [block] * count,
        in_specs=[VMEM] * (2 * count + 3),
        out_specs=[VMEM] * (count // TOGETHER + count),
        scratch_shapes=[
            pltpu.VMEM((n_exp * slots, width), BF16),
            pltpu.VMEM((n_exp * slots, hidden), BF16),
            pltpu.VMEM((tails, LANES), F32),
            pltpu.VMEM((tails, LANES), F32),
        ],
        compiler_params=params,
        name="expert",
    )(*arrived, gate_weight, up_weight, down_weight)
    came = []
    for part in results[:-count]:
        both = lax.ppermute(part, "tp", SWAP)
        came += [both[k * block.shape[0] : (k + 1) * block.shape[0]] for k in range(TOGETHER)]
    summed = [(a.astype(F32) + b.astype(F32)).astype(BF16) for a, b in zip(results[-count:], came)]
    back = exchange(summed, n_exp)
    return pl.pallas_call(
        functools.partial(combine_kernel, count=count, slots=slots),
        out_shape=jax.ShapeDtypeStruct((tok_rows // 2, width), BF16),
        in_specs=[VMEM] * (2 * count + 1),
        out_specs=VMEM,
        scratch_shapes=[
            pltpu.VMEM((left_shape[1], width), F32),
            pltpu.VMEM((n_exp * n_tail * blocks, LANES), F32),
        ],
        compiler_params=params,
        name="combine",
    )(*back, left)


def solution(mesh):
    return jax.shard_map(
        local,
        mesh=mesh,
        in_specs=(
            P(("grp", "ep"), None),
            P(),
            P("grp", "ep"),
            P("grp", "ep"),
            P("ep", None, "tp"),
            P("ep", None, "tp"),
            P("ep", "tp", None),
        ),
        out_specs=P(("grp", "ep", "tp"), None),
        check_vma=False,
    )
```

```python
import functools

import jax
import jax.numpy as jnp
from jax import lax
from jax.experimental import pallas as pl
from jax.experimental.pallas import tpu as pltpu
from jax.sharding import PartitionSpec as P


LANES = 128
SUB = 8
COPIES = 3
COVER_FLOPS = 4_000_000_000
VMEM_LIMIT = 32 * 1024 * 1024
F32 = jnp.float32
BF16 = jnp.bfloat16
SWAP = [(0, 1), (1, 0)]
VMEM = pl.BlockSpec(memory_space=pltpu.VMEM)
HBM = pl.BlockSpec(memory_space=pltpu.HBM)


def cdiv(a, b):
    return (a + b - 1) // b


def turn(core, m):
    return 1 - core if m == 0 else core


def partner(core, m, far):
    if m < far:
        return lax.axis_index("ep") ^ (2 * (far - m) + turn(core, m))
    return lax.axis_index("ep") ^ (far + 1 - m)


def pick(values, wanted):
    lane = lax.broadcasted_iota(jnp.int32, values.shape, 1)
    return jnp.sum(jnp.where(lane == wanted, values, 0.0), axis=1, keepdims=True)


def split_slots(slots):
    half_slots = slots // 2
    n_main = half_slots // SUB * SUB
    return half_slots, n_main, half_slots - n_main


def dispatch_kernel(*refs, far):
    count = far + 2
    tok_hbm, gain_hbm, rows_hbm, weight_hbm = refs[:4]
    outs = refs[4 : 4 + count]
    rows_ref, weight_ref, tok_ref, gain_ref, norm_scr, tail_scr, index_scr, sems = refs[4 + count :]
    tok_rows, width = tok_ref.shape
    slots = rows_ref.shape[1]
    step = 16
    cuts = [tok_rows * k // COPIES // step * step for k in range(COPIES)] + [tok_rows]
    copies = [
        pltpu.make_async_copy(gain_hbm, gain_ref, sems.at[COPIES]),
        pltpu.make_async_copy(rows_hbm, rows_ref, sems.at[COPIES + 1]),
        pltpu.make_async_copy(weight_hbm, weight_ref, sems.at[COPIES + 2]),
    ]
    parts = [
        pltpu.make_async_copy(tok_hbm.at[low:high], tok_ref.at[low:high], sems.at[k])
        for k, (low, high) in enumerate(zip(cuts, cuts[1:]))
    ]
    for copy in copies + parts:
        copy.start()
    for copy in copies:
        copy.wait()
    half_slots, n_main, n_tail = split_slots(slots)
    group = 2 * n_main
    blocks = width // LANES
    core = lax.axis_index("tp")
    index_scr[...] = jnp.zeros_like(index_scr)
    for m in range(count):
        index_scr[m : m + 1, :] = rows_ref[pl.ds(partner(core, m, far), 1), :]
    index = (index_scr[...] - lax.axis_index("ep") * tok_rows).astype(F32)
    sub = lax.broadcasted_iota(jnp.int32, (group, slots), 0)
    wanted = jnp.where(sub < n_main, sub, sub - n_main + half_slots)

    def one_hot(column):
        token = lax.broadcasted_iota(jnp.int32, (column.shape[0], tok_rows), 1)
        return jnp.where(token == column.astype(jnp.int32), 1.0, 0.0).astype(BF16)

    mains = [
        one_hot(pick(jnp.broadcast_to(index[m : m + 1, :], (group, slots)), wanted))
        for m in range(count)
    ]
    tails = [
        one_hot(pick(index, jnp.full(index.shape, h * half_slots + n_main + t, jnp.int32)))
        for h in range(2)
        for t in range(n_tail)
    ]
    gains = gain_ref[...].astype(F32)
    gain = jnp.concatenate([gains[j : j + 1, :] for j in range(blocks)], axis=1)
    for at in range(0, tok_rows, step):
        if at in cuts:
            parts[cuts.index(at)].wait()
        rows = slice(at, at + step)
        values = tok_ref[rows, :].astype(F32)
        scale = lax.rsqrt(jnp.mean(values * values, axis=-1, keepdims=True) + 1e-06)
        norm_scr[rows, :] = (values * scale * gain).astype(BF16)
    normed = norm_scr[...]
    together = 8
    for first in range(0, count, together):
        members = range(first, min(first + together, count))
        got = jnp.dot(
            jnp.concatenate([mains[m] for m in members], axis=0), normed, preferred_element_type=F32
        )
        for m in members:
            at = (m - first) * group
            for j in range(blocks):
                outs[m][j * group : (j + 1) * group, :] = got[
                    at : at + group, j * LANES : (j + 1) * LANES
                ].astype(BF16)
    got = jnp.dot(jnp.concatenate(tails, axis=0), normed, preferred_element_type=F32)
    padded = index.shape[0]
    per_block = 2 * n_tail * blocks
    for k in range(2 * n_tail):
        for j in range(blocks):
            tail_scr[pl.ds(k * blocks + j, padded, stride=per_block), :] = got[
                k * padded : (k + 1) * padded, j * LANES : (j + 1) * LANES
            ]
    for m in range(count):
        outs[m][group * blocks :, :] = tail_scr[m * per_block : (m + 1) * per_block, :].astype(BF16)


def expert_kernel(*refs, far, slots):
    mine, other, near = refs[:far], refs[far : 2 * far], refs[2 * far : 2 * far + 2]
    gate_ref, up_ref, down_ref = refs[2 * far + 2 : 2 * far + 5]
    rest = refs[2 * far + 5 :]
    send, keep = rest[: far + 1], rest[far + 1 : 2 * far + 2]
    x_scr, hidden_scr, tail_scr, back_scr = rest[2 * far + 2 :]
    _, width, hidden = gate_ref.shape
    n_main, n_tail = split_slots(slots)[1:]
    group = 2 * n_main
    blocks = width // LANES
    n_src = 2 * far + 2
    main_rows = n_src * group
    per_half = n_tail * blocks
    per_block = 2 * per_half
    core = lax.axis_index("tp")
    first = core == 0
    for side, base in ((mine, core * far), (other, (1 - core) * far), (near, 2 * far)):
        for m, ref in enumerate(side):
            rows = pl.ds(pl.multiple_of((base + m) * group, group), group)
            for j in range(blocks):
                x_scr[rows, j * LANES : (j + 1) * LANES] = ref[j * group : (j + 1) * group, :]
            rows = pl.ds(pl.multiple_of((base + m) * per_block, per_block), per_block)
            tail_scr[rows, :] = ref[group * blocks :, :].astype(F32)
    for j in range(blocks):
        last = [
            tail_scr[pl.ds(k * blocks + j, n_src, stride=per_block), :] for k in range(2 * n_tail)
        ]
        x_scr[main_rows:, j * LANES : (j + 1) * LANES] = jnp.concatenate(last, axis=0).astype(BF16)
    chunk = 2 * LANES
    x = x_scr[...]
    for at in range(0, hidden, chunk):
        cols = slice(at, at + chunk)
        gate = jnp.dot(x, gate_ref[0, :, cols], preferred_element_type=F32)
        up = jnp.dot(x, up_ref[0, :, cols], preferred_element_type=F32)
        hidden_scr[:, cols] = (gate / (1.0 + jnp.exp(-gate)) * up).astype(BF16)
    act = hidden_scr[...]

    def give(m, place, low, high):
        send[m][place, :] = jnp.where(first, high, low).astype(BF16)
        keep[m][place, :] = jnp.where(first, low, high).astype(BF16)

    half_rows = slots // 2 * blocks
    for at in range(0, width, chunk):
        part = jnp.dot(act, down_ref[0, :, at : at + chunk], preferred_element_type=F32)
        j = at // LANES
        for b in range(2):
            lanes = slice(b * LANES, (b + 1) * LANES)
            for m in range(far):
                low, high = (part[(s + m) * group : (s + m + 1) * group, lanes] for s in (0, far))
                give(m, slice((j + b) * group, (j + b + 1) * group), low, high)
            for k in range(2 * n_tail):
                row = main_rows + k * n_src
                back_scr[pl.ds(k * blocks + j + b, n_src, stride=per_block), :] = part[
                    row : row + n_src, lanes
                ]
        for q in range(2):
            row = (2 * far + q) * group
            low, high = (
                jnp.concatenate([part[r : r + n_main, :LANES], part[r : r + n_main, LANES:]], axis=0)
                for r in (row, row + n_main)
            )
            start = q * half_rows + j * n_main
            give(far, slice(start, start + group), low, high)
    for m in range(far):
        low, high = (back_scr[(s + m) * per_block : (s + m + 1) * per_block, :] for s in (0, far))
        give(m, slice(group * blocks, group * blocks + per_block), low, high)
    for q in range(2):
        row = (2 * far + q) * per_block
        low, high = (back_scr[r : r + per_half, :] for r in (row, row + per_half))
        start = q * half_rows + n_main * blocks
        give(far, slice(start, start + per_half), low, high)


def groups(far):
    last = (1, min(1, far - 1))
    blocks = [(side, m) for side in range(2) for m in range(far)] + [(0, far), (0, far + 1)]
    return [b for b in blocks if b != last], [last]


def depth(n_blocks, slots):
    _, n_main, n_tail = split_slots(slots)
    return n_blocks * n_main + n_tail * cdiv(n_blocks, SUB) * SUB


def route_kernel(rows_ref, weight_ref, *refs, far):
    slots = rows_ref.shape[1]
    half_slots, n_main, n_tail = split_slots(slots)
    lefts, (index_scr, weight_scr) = refs[:2], refs[2:]
    out_rows = lefts[0].shape[0] // 3
    core = lax.axis_index("tp")
    start = lax.axis_index("ep") * (2 * out_rows) + core * out_rows
    lane0 = core * half_slots
    wanted = lax.broadcasted_iota(jnp.int32, (n_main, slots), 0) + lane0

    def entry(idx, wgt):
        token = lax.broadcasted_iota(jnp.int32, (idx.shape[0], cdiv(out_rows, LANES) * LANES), 1)
        return jnp.where(token == idx.astype(jnp.int32), wgt, 0.0)

    for members, left_ref in zip(groups(far), lefts):
        padded = cdiv(len(members), SUB) * SUB
        index_scr[...] = jnp.zeros_like(index_scr)
        weight_scr[...] = jnp.zeros_like(weight_scr)
        for b, (side, m) in enumerate(members):
            row = pl.ds(partner(1 - core if side else core, m, far), 1)
            index_scr[b : b + 1, :] = rows_ref[row, :]
            weight_scr[b : b + 1, :] = weight_ref[row, :]
        index = (index_scr[:padded, :] - start).astype(F32)
        weight = weight_scr[:padded, :]
        pieces = []
        for b in range(len(members)):
            columns = [
                pick(jnp.broadcast_to(v[b : b + 1, :], (n_main, slots)), wanted)
                for v in (index, weight)
            ]
            pieces.append(entry(*columns))
        for t in range(n_tail):
            at = jnp.full((padded, slots), n_main + t, jnp.int32) + lane0
            pieces.append(entry(pick(index, at), pick(weight, at)))
        total = depth(len(members), slots)
        pieces.append(jnp.zeros((cdiv(total, LANES) * LANES - total, pieces[0].shape[1]), F32))
        pieces = [piece for piece in pieces if piece.shape[0]]
        spread = jnp.concatenate(pieces, axis=0).T[:out_rows, :]
        high = spread.astype(BF16)
        rest = spread - high.astype(F32)
        mid = rest.astype(BF16)
        low = (rest - mid.astype(F32)).astype(BF16)
        left_ref[...] = jnp.concatenate([high, mid, low], axis=0)[:, :total]


def combine_kernel(*refs, members, slots, width):
    count = len(members)
    full = slots * (width // LANES)
    sides, left_ref = refs[:count], refs[count]
    before, out_ref, row_scr, tail_scr = (None, *refs[count + 1 :])[-4:]
    out_rows = out_ref.shape[0]
    n_main, n_tail = split_slots(slots)[1:]
    blocks = width // LANES
    per_half = n_tail * blocks
    padded = cdiv(count, SUB) * SUB
    first = lax.axis_index("tp") == 0
    if padded > count:
        tail_scr[...] = jnp.zeros_like(tail_scr)
    for b, ref in enumerate(sides):
        rows = slice(b * n_main, (b + 1) * n_main)
        whole = ref.shape[0] == full
        for j in range(0, blocks, 2):
            if whole:
                pair = [
                    ref[k * 2 * n_main : (k + 1) * 2 * n_main, :].astype(F32) for k in (j, j + 1)
                ]
                pair = [jnp.where(first, two[:n_main], two[n_main:]) for two in pair]
            else:
                two = ref[j * n_main : (j + 2) * n_main, :].astype(F32)
                pair = [two[:n_main], two[n_main:]]
            for k in range(2):
                row_scr[rows, (j + k) * LANES : (j + k + 1) * LANES] = pair[k]
        if whole:
            two = ref[2 * n_main * blocks :, :].astype(F32)
            two = jnp.where(first, two[:per_half], two[per_half:])
        else:
            two = ref[n_main * blocks :, :].astype(F32)
        tail_scr[b * per_half : (b + 1) * per_half, :] = two
    for t in range(n_tail):
        rows = slice(count * n_main + t * padded, count * n_main + (t + 1) * padded)
        for j in range(blocks):
            row_scr[rows, j * LANES : (j + 1) * LANES] = tail_scr[
                pl.ds(t * blocks + j, padded, stride=per_half), :
            ]
    left = left_ref[...]
    chunk = 2 * LANES
    for at in range(0, width, chunk):
        cols = slice(at, at + chunk)
        got = jnp.dot(left, row_scr[:, cols].astype(BF16), preferred_element_type=F32)
        got = got[:out_rows] + (got[out_rows : 2 * out_rows] + got[2 * out_rows :])
        if before is not None:
            got = before[:, cols] + got
        out_ref[:, cols] = got.astype(out_ref.dtype)


def exchange(blocks, n_exp):
    far = len(blocks) - 1
    came, passed = [], []
    for m, block in enumerate(blocks):
        gap = [2 * (far - m) + turn(c, m) if m < far else 1 for c in range(2)]
        pairs = [(2 * e + c, 2 * (e ^ gap[c]) + c) for e in range(n_exp) for c in range(2)]
        came.append(lax.ppermute(block, ("ep", "tp"), pairs))
    for block in came[:far]:
        passed.append(lax.ppermute(block, "tp", SWAP))
    return came[:far], passed, came[far]


def local(tokens, norm_gain, chosen_rows, route_weights, gate_weight, up_weight, down_weight):
    tok_rows, width = tokens.shape
    n_exp, slots = chosen_rows.shape
    _, n_tail = split_slots(slots)[1:]
    far = n_exp // 2 - 1
    hidden = gate_weight.shape[2]
    blocks = width // LANES
    block = jax.ShapeDtypeStruct((slots * blocks, LANES), BF16)
    padded = cdiv(far + 2, SUB) * SUB
    args = (tokens, norm_gain.reshape(blocks, LANES), chosen_rows, route_weights)
    params = pltpu.CompilerParams(vmem_limit_bytes=VMEM_LIMIT)
    *outgoing, own, own_rows, own_weights = pl.pallas_call(
        functools.partial(dispatch_kernel, far=far),
        out_shape=[block] * (far + 2)
        + [jax.ShapeDtypeStruct(x.shape, x.dtype) for x in (chosen_rows, route_weights)],
        in_specs=[HBM] * 4,
        out_specs=[VMEM] * (far + 4),
        scratch_shapes=[
            pltpu.VMEM((tok_rows, width), BF16),
            pltpu.VMEM((blocks, LANES), BF16),
            pltpu.VMEM((tok_rows, width), BF16),
            pltpu.VMEM((padded * 2 * n_tail * blocks, LANES), F32),
            pltpu.VMEM((padded, slots), jnp.int32),
            pltpu.SemaphoreType.DMA((COPIES + 3,)),
        ],
        compiler_params=params,
        name="dispatch",
    )(*(pltpu.with_memory_space_constraint(x, pltpu.HBM) for x in args))
    out_rows = tok_rows // 2
    members = groups(far)
    depths = [depth(len(m), slots) for m in members]
    weight_bytes = 3 * 2 * width * hidden
    most = cdiv(len(members[0]), SUB) * SUB
    lefts = pl.pallas_call(
        functools.partial(route_kernel, far=far),
        out_shape=[jax.ShapeDtypeStruct((3 * out_rows, d), BF16) for d in depths],
        in_specs=[VMEM] * 2,
        out_specs=[VMEM] * 2,
        scratch_shapes=[pltpu.VMEM((most, slots), jnp.int32), pltpu.VMEM((most, slots), F32)],
        compiler_params=params,
        cost_estimate=pl.CostEstimate(
            flops=COVER_FLOPS, bytes_accessed=weight_bytes, transcendentals=0
        ),
        name="route",
    )(own_rows, own_weights)
    mine, other, near = exchange(outgoing, n_exp)
    tails = n_exp * 2 * n_tail * blocks
    results = pl.pallas_call(
        functools.partial(expert_kernel, far=far, slots=slots),
        out_shape=[block] * (2 * far + 2),
        in_specs=[VMEM] * (2 * far + 5),
        out_specs=[VMEM] * (2 * far + 2),
        scratch_shapes=[
            pltpu.VMEM((n_exp * slots, width), BF16),
            pltpu.VMEM((n_exp * slots, hidden), BF16),
            pltpu.VMEM((tails, LANES), F32),
            pltpu.VMEM((tails, LANES), F32),
        ],
        compiler_params=params,
        name="expert",
    )(*mine, *other, near, own, gate_weight, up_weight, down_weight)
    came = []
    for part in results[: far + 1]:
        came.append(lax.ppermute(part, "tp", SWAP))

    def add(a, b):
        return (a.astype(F32) + b.astype(F32)).astype(BF16)

    summed = [add(a, b) for a, b in zip(results[far + 1 : -1], came)]
    half = slots // 2 * blocks
    neighbour, own = (add(results[-1][rows], came[-1][rows]) for rows in (slice(0, half), slice(half, None)))
    mine, other, near = exchange(summed + [neighbour], n_exp)
    sides = ([*mine, near, own], other)
    total = None
    for k, (blocks_in, left) in enumerate(zip(members, lefts)):
        final = k == len(members) - 1
        ins = [sides[side][m] for side, m in blocks_in] + [left] + ([] if total is None else [total])
        total = pl.pallas_call(
            functools.partial(combine_kernel, members=blocks_in, slots=slots, width=width),
            out_shape=jax.ShapeDtypeStruct((out_rows, width), BF16 if final else F32),
            in_specs=[VMEM] * len(ins),
            out_specs=VMEM,
            scratch_shapes=[
                pltpu.VMEM((depths[k], width), F32),
                pltpu.VMEM((cdiv(len(blocks_in), SUB) * SUB * n_tail * blocks, LANES), F32),
            ],
            compiler_params=params,
        )(*ins)
    return total


def solution(mesh):
    return jax.shard_map(
        local,
        mesh=mesh,
        in_specs=(
            P(("grp", "ep"), None),
            P(),
            P("grp", "ep"),
            P("grp", "ep"),
            P("ep", None, "tp"),
            P("ep", None, "tp"),
            P("ep", "tp", None),
        ),
        out_specs=P(("grp", "ep", "tp"), None),
        check_vma=False,
    )
```

```python
import functools

import jax
import jax.numpy as jnp
from jax import lax
from jax.experimental import pallas as pl
from jax.experimental.pallas import tpu as pltpu
from jax.sharding import PartitionSpec as P


LANES = 128
SUB = 8
COPIES = 1
OUT_COPIES = 4
COVER_FLOPS = 4_000_000_000
VMEM_LIMIT = 32 * 1024 * 1024
F32 = jnp.float32
BF16 = jnp.bfloat16
SWAP = [(0, 1), (1, 0)]
VMEM = pl.BlockSpec(memory_space=pltpu.VMEM)
HBM = pl.BlockSpec(memory_space=pltpu.HBM)


def cdiv(a, b):
    return (a + b - 1) // b


def turn(core, m):
    return 1 - core if m == 0 else core


def partner(core, m, far):
    if m < far:
        return lax.axis_index("ep") ^ (2 * (far - m) + turn(core, m))
    return lax.axis_index("ep") ^ (far + 1 - m)


def pick(values, wanted):
    lane = lax.broadcasted_iota(jnp.int32, values.shape, 1)
    return jnp.sum(jnp.where(lane == wanted, values, 0.0), axis=1, keepdims=True)


def split_slots(slots):
    half_slots = slots // 2
    n_main = half_slots // SUB * SUB
    return half_slots, n_main, half_slots - n_main


def dispatch_kernel(*refs, far):
    count = far + 2
    tok_hbm, gain_hbm, rows_hbm, weight_hbm = refs[:4]
    outs = refs[4 : 4 + count]
    rows_ref, weight_ref, tok_ref, gain_ref, norm_scr, tail_scr, index_scr, sems = refs[4 + count :]
    tok_rows, width = tok_ref.shape
    slots = rows_ref.shape[1]
    step = 16
    cuts = [tok_rows * k // COPIES // step * step for k in range(COPIES)] + [tok_rows]
    copies = [
        pltpu.make_async_copy(gain_hbm, gain_ref, sems.at[COPIES]),
        pltpu.make_async_copy(rows_hbm, rows_ref, sems.at[COPIES + 1]),
        pltpu.make_async_copy(weight_hbm, weight_ref, sems.at[COPIES + 2]),
    ]
    parts = [
        pltpu.make_async_copy(tok_hbm.at[low:high], tok_ref.at[low:high], sems.at[k])
        for k, (low, high) in enumerate(zip(cuts, cuts[1:]))
    ]
    for copy in copies + parts:
        copy.start()
    for copy in copies + parts:
        copy.wait()
    half_slots, n_main, n_tail = split_slots(slots)
    group = 2 * n_main
    blocks = width // LANES
    core = lax.axis_index("tp")
    index_scr[...] = jnp.zeros_like(index_scr)
    for m in range(count):
        index_scr[m : m + 1, :] = rows_ref[pl.ds(partner(core, m, far), 1), :]
    index = (index_scr[...] - lax.axis_index("ep") * tok_rows).astype(F32)
    sub = lax.broadcasted_iota(jnp.int32, (group, slots), 0)
    wanted = jnp.where(sub < n_main, sub, sub - n_main + half_slots)

    def one_hot(column):
        token = lax.broadcasted_iota(jnp.int32, (column.shape[0], tok_rows), 1)
        return jnp.where(token == column.astype(jnp.int32), 1.0, 0.0).astype(BF16)

    mains = [
        one_hot(pick(jnp.broadcast_to(index[m : m + 1, :], (group, slots)), wanted))
        for m in range(count)
    ]
    tails = [
        one_hot(pick(index, jnp.full(index.shape, h * half_slots + n_main + t, jnp.int32)))
        for h in range(2)
        for t in range(n_tail)
    ]
    gains = gain_ref[...].astype(F32)
    gain = jnp.concatenate([gains[j : j + 1, :] for j in range(blocks)], axis=1)
    for at in range(0, tok_rows, step):
        rows = slice(at, at + step)
        values = tok_ref[rows, :].astype(F32)
        scale = lax.rsqrt(jnp.mean(values * values, axis=-1, keepdims=True) + 1e-06)
        norm_scr[rows, :] = (values * scale * gain).astype(BF16)
    left = jnp.concatenate(mains + tails, axis=0)
    padded = index.shape[0]
    per_block = 2 * n_tail * blocks
    chunk = 2 * LANES
    for at in range(0, width, chunk):
        got = jnp.dot(left, norm_scr[:, at : at + chunk], preferred_element_type=F32)
        for b in range(chunk // LANES):
            lanes = slice(b * LANES, (b + 1) * LANES)
            j = at // LANES + b
            for m in range(count):
                outs[m][j * group : (j + 1) * group, :] = got[
                    m * group : (m + 1) * group, lanes
                ].astype(BF16)
            for k in range(2 * n_tail):
                row = count * group + k * padded
                tail_scr[pl.ds(k * blocks + j, padded, stride=per_block), :] = got[
                    row : row + padded, lanes
                ]
    for m in range(count):
        outs[m][group * blocks :, :] = tail_scr[m * per_block : (m + 1) * per_block, :].astype(BF16)


def expert_kernel(*refs, far, slots):
    mine, other, near = refs[:far], refs[far : 2 * far], refs[2 * far : 2 * far + 2]
    gate_ref, up_ref, down_ref = refs[2 * far + 2 : 2 * far + 5]
    rest = refs[2 * far + 5 :]
    send, keep = rest[: far + 1], rest[far + 1 : 2 * far + 2]
    x_scr, hidden_scr, tail_scr, back_scr = rest[2 * far + 2 :]
    _, width, hidden = gate_ref.shape
    n_main, n_tail = split_slots(slots)[1:]
    group = 2 * n_main
    blocks = width // LANES
    n_src = 2 * far + 2
    main_rows = n_src * group
    per_half = n_tail * blocks
    per_block = 2 * per_half
    core = lax.axis_index("tp")
    first = core == 0
    for side, base in ((mine, core * far), (other, (1 - core) * far), (near, 2 * far)):
        for m, ref in enumerate(side):
            rows = pl.ds(pl.multiple_of((base + m) * group, group), group)
            for j in range(blocks):
                x_scr[rows, j * LANES : (j + 1) * LANES] = ref[j * group : (j + 1) * group, :]
            rows = pl.ds(pl.multiple_of((base + m) * per_block, per_block), per_block)
            tail_scr[rows, :] = ref[group * blocks :, :].astype(F32)
    for j in range(blocks):
        last = [
            tail_scr[pl.ds(k * blocks + j, n_src, stride=per_block), :] for k in range(2 * n_tail)
        ]
        x_scr[main_rows:, j * LANES : (j + 1) * LANES] = jnp.concatenate(last, axis=0).astype(BF16)
    chunk = 2 * LANES
    x = x_scr[...]
    for at in range(0, hidden, chunk):
        cols = slice(at, at + chunk)
        gate = jnp.dot(x, gate_ref[0, :, cols], preferred_element_type=F32)
        up = jnp.dot(x, up_ref[0, :, cols], preferred_element_type=F32)
        hidden_scr[:, cols] = (gate / (1.0 + jnp.exp(-gate)) * up).astype(BF16)
    act = hidden_scr[...]

    def give(m, place, low, high):
        send[m][place, :] = jnp.where(first, high, low).astype(BF16)
        keep[m][place, :] = jnp.where(first, low, high).astype(BF16)

    half_rows = slots // 2 * blocks
    for at in range(0, width, chunk):
        part = jnp.dot(act, down_ref[0, :, at : at + chunk], preferred_element_type=F32)
        j = at // LANES
        for b in range(2):
            lanes = slice(b * LANES, (b + 1) * LANES)
            for m in range(far):
                low, high = (part[(s + m) * group : (s + m + 1) * group, lanes] for s in (0, far))
                give(m, slice((j + b) * group, (j + b + 1) * group), low, high)
            for k in range(2 * n_tail):
                row = main_rows + k * n_src
                back_scr[pl.ds(k * blocks + j + b, n_src, stride=per_block), :] = part[
                    row : row + n_src, lanes
                ]
        for q in range(2):
            row = (2 * far + q) * group
            low, high = (
                jnp.concatenate([part[r : r + n_main, :LANES], part[r : r + n_main, LANES:]], axis=0)
                for r in (row, row + n_main)
            )
            start = q * half_rows + j * n_main
            give(far, slice(start, start + group), low, high)
    for m in range(far):
        low, high = (back_scr[(s + m) * per_block : (s + m + 1) * per_block, :] for s in (0, far))
        give(m, slice(group * blocks, group * blocks + per_block), low, high)
    for q in range(2):
        row = (2 * far + q) * per_block
        low, high = (back_scr[r : r + per_half, :] for r in (row, row + per_half))
        start = q * half_rows + n_main * blocks
        give(far, slice(start, start + per_half), low, high)


def groups(far):
    last = (1, min(1, far - 1))
    blocks = [(side, m) for side in range(2) for m in range(far)] + [(0, far), (0, far + 1)]
    return [b for b in blocks if b != last], [last]


def depth(n_blocks, slots):
    _, n_main, n_tail = split_slots(slots)
    return n_blocks * n_main + n_tail * cdiv(n_blocks, SUB) * SUB


def route_kernel(rows_ref, weight_ref, *refs, far):
    slots = rows_ref.shape[1]
    half_slots, n_main, n_tail = split_slots(slots)
    lefts, (index_scr, weight_scr) = refs[:2], refs[2:]
    out_rows = lefts[0].shape[0] // 3
    core = lax.axis_index("tp")
    start = lax.axis_index("ep") * (2 * out_rows) + core * out_rows
    lane0 = core * half_slots
    wanted = lax.broadcasted_iota(jnp.int32, (n_main, slots), 0) + lane0

    def entry(idx, wgt):
        token = lax.broadcasted_iota(jnp.int32, (idx.shape[0], cdiv(out_rows, LANES) * LANES), 1)
        return jnp.where(token == idx.astype(jnp.int32), wgt, 0.0)

    for members, left_ref in zip(groups(far), lefts):
        padded = cdiv(len(members), SUB) * SUB
        index_scr[...] = jnp.zeros_like(index_scr)
        weight_scr[...] = jnp.zeros_like(weight_scr)
        for b, (side, m) in enumerate(members):
            row = pl.ds(partner(1 - core if side else core, m, far), 1)
            index_scr[b : b + 1, :] = rows_ref[row, :]
            weight_scr[b : b + 1, :] = weight_ref[row, :]
        index = (index_scr[:padded, :] - start).astype(F32)
        weight = weight_scr[:padded, :]
        pieces = []
        for b in range(len(members)):
            columns = [
                pick(jnp.broadcast_to(v[b : b + 1, :], (n_main, slots)), wanted)
                for v in (index, weight)
            ]
            pieces.append(entry(*columns))
        for t in range(n_tail):
            at = jnp.full((padded, slots), n_main + t, jnp.int32) + lane0
            pieces.append(entry(pick(index, at), pick(weight, at)))
        total = depth(len(members), slots)
        pieces.append(jnp.zeros((cdiv(total, LANES) * LANES - total, pieces[0].shape[1]), F32))
        pieces = [piece for piece in pieces if piece.shape[0]]
        spread = jnp.concatenate(pieces, axis=0).T[:out_rows, :]
        high = spread.astype(BF16)
        rest = spread - high.astype(F32)
        mid = rest.astype(BF16)
        low = (rest - mid.astype(F32)).astype(BF16)
        left_ref[...] = jnp.concatenate([high, mid, low], axis=0)[:, :total]


def combine_kernel(*refs, members, slots, width, copies):
    count = len(members)
    full = slots * (width // LANES)
    sides, left_ref = refs[:count], refs[count]
    rest = refs[count + 1 :]
    before = None
    if copies:
        before, out_hbm, row_scr, tail_scr, out_ref, sems = rest
    else:
        out_ref, row_scr, tail_scr = rest
    out_rows = out_ref.shape[0]
    n_main, n_tail = split_slots(slots)[1:]
    blocks = width // LANES
    per_half = n_tail * blocks
    padded = cdiv(count, SUB) * SUB
    first = lax.axis_index("tp") == 0
    if padded > count:
        tail_scr[...] = jnp.zeros_like(tail_scr)
    for b, ref in enumerate(sides):
        rows = slice(b * n_main, (b + 1) * n_main)
        whole = ref.shape[0] == full
        for j in range(0, blocks, 2):
            if whole:
                pair = [
                    ref[k * 2 * n_main : (k + 1) * 2 * n_main, :].astype(F32) for k in (j, j + 1)
                ]
                pair = [jnp.where(first, two[:n_main], two[n_main:]) for two in pair]
            else:
                two = ref[j * n_main : (j + 2) * n_main, :].astype(F32)
                pair = [two[:n_main], two[n_main:]]
            for k in range(2):
                row_scr[rows, (j + k) * LANES : (j + k + 1) * LANES] = pair[k]
        if whole:
            two = ref[2 * n_main * blocks :, :].astype(F32)
            two = jnp.where(first, two[:per_half], two[per_half:])
        else:
            two = ref[n_main * blocks :, :].astype(F32)
        tail_scr[b * per_half : (b + 1) * per_half, :] = two
    for t in range(n_tail):
        rows = slice(count * n_main + t * padded, count * n_main + (t + 1) * padded)
        for j in range(blocks):
            row_scr[rows, j * LANES : (j + 1) * LANES] = tail_scr[
                pl.ds(t * blocks + j, padded, stride=per_half), :
            ]
    left = left_ref[...]
    chunk = 2 * LANES
    started = []
    for at in range(0, width, chunk):
        cols = slice(at, at + chunk)
        got = jnp.dot(left, row_scr[:, cols].astype(BF16), preferred_element_type=F32)
        got = got[:out_rows] + (got[out_rows : 2 * out_rows] + got[2 * out_rows :])
        if before is not None:
            got = before[:, cols] + got
        out_ref[:, cols] = got.astype(out_ref.dtype)
        if copies and (at + chunk) % (width // copies) == 0:
            cols = slice(at + chunk - width // copies, at + chunk)
            started.append(
                pltpu.make_async_copy(
                    out_ref.at[:, cols], out_hbm.at[:, cols], sems.at[len(started)]
                )
            )
            started[-1].start()
    for copy in started:
        copy.wait()


def exchange(blocks, n_exp):
    far = len(blocks) - 1
    came, passed = [], []
    for m, block in enumerate(blocks):
        gap = [2 * (far - m) + turn(c, m) if m < far else 1 for c in range(2)]
        pairs = [(2 * e + c, 2 * (e ^ gap[c]) + c) for e in range(n_exp) for c in range(2)]
        came.append(lax.ppermute(block, ("ep", "tp"), pairs))
    for block in came[:far]:
        passed.append(lax.ppermute(block, "tp", SWAP))
    return came[:far], passed, came[far]


def local(tokens, norm_gain, chosen_rows, route_weights, gate_weight, up_weight, down_weight):
    tok_rows, width = tokens.shape
    n_exp, slots = chosen_rows.shape
    _, n_tail = split_slots(slots)[1:]
    far = n_exp // 2 - 1
    hidden = gate_weight.shape[2]
    blocks = width // LANES
    block = jax.ShapeDtypeStruct((slots * blocks, LANES), BF16)
    padded = cdiv(far + 2, SUB) * SUB
    args = (tokens, norm_gain.reshape(blocks, LANES), chosen_rows, route_weights)
    params = pltpu.CompilerParams(vmem_limit_bytes=VMEM_LIMIT)
    *outgoing, own, own_rows, own_weights = pl.pallas_call(
        functools.partial(dispatch_kernel, far=far),
        out_shape=[block] * (far + 2)
        + [jax.ShapeDtypeStruct(x.shape, x.dtype) for x in (chosen_rows, route_weights)],
        in_specs=[HBM] * 4,
        out_specs=[VMEM] * (far + 4),
        scratch_shapes=[
            pltpu.VMEM((tok_rows, width), BF16),
            pltpu.VMEM((blocks, LANES), BF16),
            pltpu.VMEM((tok_rows, width), BF16),
            pltpu.VMEM((padded * 2 * n_tail * blocks, LANES), F32),
            pltpu.VMEM((padded, slots), jnp.int32),
            pltpu.SemaphoreType.DMA((COPIES + 3,)),
        ],
        compiler_params=params,
        name="dispatch",
    )(*(pltpu.with_memory_space_constraint(x, pltpu.HBM) for x in args))
    out_rows = tok_rows // 2
    members = groups(far)
    depths = [depth(len(m), slots) for m in members]
    weight_bytes = 3 * 2 * width * hidden
    most = cdiv(len(members[0]), SUB) * SUB
    lefts = pl.pallas_call(
        functools.partial(route_kernel, far=far),
        out_shape=[jax.ShapeDtypeStruct((3 * out_rows, d), BF16) for d in depths],
        in_specs=[VMEM] * 2,
        out_specs=[VMEM] * 2,
        scratch_shapes=[pltpu.VMEM((most, slots), jnp.int32), pltpu.VMEM((most, slots), F32)],
        compiler_params=params,
        cost_estimate=pl.CostEstimate(
            flops=COVER_FLOPS, bytes_accessed=weight_bytes, transcendentals=0
        ),
        name="route",
    )(own_rows, own_weights)
    mine, other, near = exchange(outgoing, n_exp)
    tails = n_exp * 2 * n_tail * blocks
    results = pl.pallas_call(
        functools.partial(expert_kernel, far=far, slots=slots),
        out_shape=[block] * (2 * far + 2),
        in_specs=[VMEM] * (2 * far + 5),
        out_specs=[VMEM] * (2 * far + 2),
        scratch_shapes=[
            pltpu.VMEM((n_exp * slots, width), BF16),
            pltpu.VMEM((n_exp * slots, hidden), BF16),
            pltpu.VMEM((tails, LANES), F32),
            pltpu.VMEM((tails, LANES), F32),
        ],
        compiler_params=params,
        name="expert",
    )(*mine, *other, near, own, gate_weight, up_weight, down_weight)
    came = []
    for part in results[: far + 1]:
        came.append(lax.ppermute(part, "tp", SWAP))

    def add(a, b):
        return (a.astype(F32) + b.astype(F32)).astype(BF16)

    summed = [add(a, b) for a, b in zip(results[far + 1 : -1], came)]
    half = slots // 2 * blocks
    neighbour, own = (add(results[-1][rows], came[-1][rows]) for rows in (slice(0, half), slice(half, None)))
    mine, other, near = exchange(summed + [neighbour], n_exp)
    sides = ([*mine, near, own], other)
    total = None
    for k, (blocks_in, left) in enumerate(zip(members, lefts)):
        final = k == len(members) - 1
        ins = [sides[side][m] for side, m in blocks_in] + [left] + ([] if total is None else [total])
        total = pl.pallas_call(
            functools.partial(
                combine_kernel,
                members=blocks_in,
                slots=slots,
                width=width,
                copies=OUT_COPIES if final else 0,
            ),
            out_shape=jax.ShapeDtypeStruct((out_rows, width), BF16 if final else F32),
            in_specs=[VMEM] * len(ins),
            out_specs=pl.BlockSpec(memory_space=pl.ANY) if final else VMEM,
            scratch_shapes=[
                pltpu.VMEM((depths[k], width), F32),
                pltpu.VMEM((cdiv(len(blocks_in), SUB) * SUB * n_tail * blocks, LANES), F32),
            ]
            + [pltpu.VMEM((out_rows, width), BF16), pltpu.SemaphoreType.DMA((OUT_COPIES,))] * final,
            compiler_params=params,
        )(*ins)
    return total


def solution(mesh):
    return jax.shard_map(
        local,
        mesh=mesh,
        in_specs=(
            P(("grp", "ep"), None),
            P(),
            P("grp", "ep"),
            P("grp", "ep"),
            P("ep", None, "tp"),
            P("ep", None, "tp"),
            P("ep", "tp", None),
        ),
        out_specs=P(("grp", "ep", "tp"), None),
        check_vma=False,
    )
```

```python
import functools

import jax
import jax.numpy as jnp
from jax import lax
from jax.experimental import pallas as pl
from jax.experimental.pallas import tpu as pltpu
from jax.sharding import PartitionSpec as P


LANES = 128
SUB = 8
COPIES = 1
OUT_COPIES = 4
COVER_FLOPS = 4_000_000_000
VMEM_LIMIT = 32 * 1024 * 1024
F32 = jnp.float32
BF16 = jnp.bfloat16
SWAP = [(0, 1), (1, 0)]
VMEM = pl.BlockSpec(memory_space=pltpu.VMEM)
HBM = pl.BlockSpec(memory_space=pltpu.HBM)


def cdiv(a, b):
    return (a + b - 1) // b


def turn(core, m):
    return 1 - core if m == 0 else core


def partner(core, m, far):
    if m < far:
        return lax.axis_index("ep") ^ (2 * (far - m) + turn(core, m))
    return lax.axis_index("ep") ^ (far + 1 - m)


def pick(values, wanted):
    lane = lax.broadcasted_iota(jnp.int32, values.shape, 1)
    return jnp.sum(jnp.where(lane == wanted, values, 0.0), axis=1, keepdims=True)


def split_slots(slots):
    half_slots = slots // 2
    n_main = half_slots // SUB * SUB
    return half_slots, n_main, half_slots - n_main


def dispatch_kernel(*refs, far):
    count = far + 2
    tok_hbm, gain_hbm, rows_hbm, weight_hbm = refs[:4]
    outs = refs[4 : 4 + count]
    rows_ref, weight_ref, tok_ref, gain_ref, norm_scr, tail_scr, index_scr, sems = refs[4 + count :]
    tok_rows, width = tok_ref.shape
    slots = rows_ref.shape[1]
    step = 16
    cuts = [tok_rows * k // COPIES // step * step for k in range(COPIES)] + [tok_rows]
    copies = [
        pltpu.make_async_copy(gain_hbm, gain_ref, sems.at[COPIES]),
        pltpu.make_async_copy(rows_hbm, rows_ref, sems.at[COPIES + 1]),
        pltpu.make_async_copy(weight_hbm, weight_ref, sems.at[COPIES + 2]),
    ]
    parts = [
        pltpu.make_async_copy(tok_hbm.at[low:high], tok_ref.at[low:high], sems.at[k])
        for k, (low, high) in enumerate(zip(cuts, cuts[1:]))
    ]
    for copy in copies + parts:
        copy.start()
    for copy in copies + parts:
        copy.wait()
    half_slots, n_main, n_tail = split_slots(slots)
    group = 2 * n_main
    blocks = width // LANES
    core = lax.axis_index("tp")
    index_scr[...] = jnp.zeros_like(index_scr)
    for m in range(count):
        index_scr[m : m + 1, :] = rows_ref[pl.ds(partner(core, m, far), 1), :]
    index = (index_scr[...] - lax.axis_index("ep") * tok_rows).astype(F32)
    sub = lax.broadcasted_iota(jnp.int32, (group, slots), 0)
    wanted = jnp.where(sub < n_main, sub, sub - n_main + half_slots)

    def one_hot(column):
        token = lax.broadcasted_iota(jnp.int32, (column.shape[0], tok_rows), 1)
        return jnp.where(token == column.astype(jnp.int32), 1.0, 0.0).astype(BF16)

    mains = [
        one_hot(pick(jnp.broadcast_to(index[m : m + 1, :], (group, slots)), wanted))
        for m in range(count)
    ]
    tails = [
        one_hot(pick(index, jnp.full(index.shape, h * half_slots + n_main + t, jnp.int32)))
        for h in range(2)
        for t in range(n_tail)
    ]
    gains = gain_ref[...].astype(F32)
    gain = jnp.concatenate([gains[j : j + 1, :] for j in range(blocks)], axis=1)
    for at in range(0, tok_rows, step):
        rows = slice(at, at + step)
        values = tok_ref[rows, :].astype(F32)
        scale = lax.rsqrt(jnp.mean(values * values, axis=-1, keepdims=True) + 1e-06)
        norm_scr[rows, :] = (values * scale * gain).astype(BF16)
    left = jnp.concatenate(mains + tails, axis=0)
    padded = index.shape[0]
    per_block = 2 * n_tail * blocks
    chunk = 2 * LANES
    for at in range(0, width, chunk):
        got = jnp.dot(left, norm_scr[:, at : at + chunk], preferred_element_type=F32)
        for b in range(chunk // LANES):
            lanes = slice(b * LANES, (b + 1) * LANES)
            j = at // LANES + b
            for m in range(count):
                outs[m][j * group : (j + 1) * group, :] = got[
                    m * group : (m + 1) * group, lanes
                ].astype(BF16)
            for k in range(2 * n_tail):
                row = count * group + k * padded
                tail_scr[pl.ds(k * blocks + j, padded, stride=per_block), :] = got[
                    row : row + padded, lanes
                ]
    for m in range(count):
        outs[m][group * blocks :, :] = tail_scr[m * per_block : (m + 1) * per_block, :].astype(BF16)


def expert_kernel(*refs, far, slots):
    mine, other, near = refs[:far], refs[far : 2 * far], refs[2 * far : 2 * far + 2]
    gate_ref, up_ref, down_ref = refs[2 * far + 2 : 2 * far + 5]
    rest = refs[2 * far + 5 :]
    send, keep = rest[: far + 1], rest[far + 1 : 2 * far + 2]
    x_scr, hidden_scr, tail_scr, back_scr = rest[2 * far + 2 :]
    _, width, hidden = gate_ref.shape
    n_main, n_tail = split_slots(slots)[1:]
    group = 2 * n_main
    blocks = width // LANES
    n_src = 2 * far + 2
    main_rows = n_src * group
    per_half = n_tail * blocks
    per_block = 2 * per_half
    core = lax.axis_index("tp")
    first = core == 0
    for side, base in ((mine, core * far), (other, (1 - core) * far), (near, 2 * far)):
        for m, ref in enumerate(side):
            rows = pl.ds(pl.multiple_of((base + m) * group, group), group)
            for j in range(blocks):
                x_scr[rows, j * LANES : (j + 1) * LANES] = ref[j * group : (j + 1) * group, :]
            rows = pl.ds(pl.multiple_of((base + m) * per_block, per_block), per_block)
            tail_scr[rows, :] = ref[group * blocks :, :].astype(F32)
    for j in range(blocks):
        last = [
            tail_scr[pl.ds(k * blocks + j, n_src, stride=per_block), :] for k in range(2 * n_tail)
        ]
        x_scr[main_rows:, j * LANES : (j + 1) * LANES] = jnp.concatenate(last, axis=0).astype(BF16)
    chunk = 2 * LANES
    x = x_scr[...]
    for at in range(0, hidden, chunk):
        cols = slice(at, at + chunk)
        gate = jnp.dot(x, gate_ref[0, :, cols], preferred_element_type=F32)
        up = jnp.dot(x, up_ref[0, :, cols], preferred_element_type=F32)
        hidden_scr[:, cols] = (gate / (1.0 + jnp.exp(-gate)) * up).astype(BF16)
    act = hidden_scr[...]

    def give(m, place, low, high):
        send[m][place, :] = jnp.where(first, high, low).astype(BF16)
        keep[m][place, :] = jnp.where(first, low, high).astype(BF16)

    half_rows = slots // 2 * blocks
    for at in range(0, width, chunk):
        part = jnp.dot(act, down_ref[0, :, at : at + chunk], preferred_element_type=F32)
        j = at // LANES
        for b in range(2):
            lanes = slice(b * LANES, (b + 1) * LANES)
            for m in range(far):
                low, high = (part[(s + m) * group : (s + m + 1) * group, lanes] for s in (0, far))
                give(m, slice((j + b) * group, (j + b + 1) * group), low, high)
            for k in range(2 * n_tail):
                row = main_rows + k * n_src
                back_scr[pl.ds(k * blocks + j + b, n_src, stride=per_block), :] = part[
                    row : row + n_src, lanes
                ]
        for q in range(2):
            row = (2 * far + q) * group
            low, high = (
                jnp.concatenate([part[r : r + n_main, :LANES], part[r : r + n_main, LANES:]], axis=0)
                for r in (row, row + n_main)
            )
            start = q * half_rows + j * n_main
            give(far, slice(start, start + group), low, high)
    for m in range(far):
        low, high = (back_scr[(s + m) * per_block : (s + m + 1) * per_block, :] for s in (0, far))
        give(m, slice(group * blocks, group * blocks + per_block), low, high)
    for q in range(2):
        row = (2 * far + q) * per_block
        low, high = (back_scr[r : r + per_half, :] for r in (row, row + per_half))
        start = q * half_rows + n_main * blocks
        give(far, slice(start, start + per_half), low, high)


def groups(far):
    last = (1, min(1, far - 1))
    blocks = [(side, m) for side in range(2) for m in range(far)] + [(0, far), (0, far + 1)]
    return [b for b in blocks if b != last], [last]


def depth(n_blocks, slots):
    _, n_main, n_tail = split_slots(slots)
    return n_blocks * n_main + n_tail * cdiv(n_blocks, SUB) * SUB


def route_kernel(rows_ref, weight_ref, *refs, far):
    slots = rows_ref.shape[1]
    half_slots, n_main, n_tail = split_slots(slots)
    lefts, (index_scr, weight_scr) = refs[:2], refs[2:]
    out_rows = lefts[0].shape[0]
    core = lax.axis_index("tp")
    start = lax.axis_index("ep") * (2 * out_rows) + core * out_rows
    lane0 = core * half_slots
    wanted = lax.broadcasted_iota(jnp.int32, (n_main, slots), 0) + lane0

    def entry(idx, wgt):
        token = lax.broadcasted_iota(jnp.int32, (idx.shape[0], cdiv(out_rows, LANES) * LANES), 1)
        return jnp.where(token == idx.astype(jnp.int32), wgt, 0.0)

    for members, left_ref in zip(groups(far), lefts):
        padded = cdiv(len(members), SUB) * SUB
        index_scr[...] = jnp.zeros_like(index_scr)
        weight_scr[...] = jnp.zeros_like(weight_scr)
        for b, (side, m) in enumerate(members):
            row = pl.ds(partner(1 - core if side else core, m, far), 1)
            index_scr[b : b + 1, :] = rows_ref[row, :]
            weight_scr[b : b + 1, :] = weight_ref[row, :]
        index = (index_scr[:padded, :] - start).astype(F32)
        weight = weight_scr[:padded, :]
        pieces = []
        for b in range(len(members)):
            columns = [
                pick(jnp.broadcast_to(v[b : b + 1, :], (n_main, slots)), wanted)
                for v in (index, weight)
            ]
            pieces.append(entry(*columns))
        for t in range(n_tail):
            at = jnp.full((padded, slots), n_main + t, jnp.int32) + lane0
            pieces.append(entry(pick(index, at), pick(weight, at)))
        spread = jnp.concatenate(pieces, axis=0)
        high = spread.astype(BF16).astype(F32)
        mid = (spread - high).astype(BF16).astype(F32)
        parts = [high, mid, spread - high - mid]
        total = 3 * depth(len(members), slots)
        missing = cdiv(total, LANES) * LANES - total
        if missing:
            parts.append(jnp.zeros((missing, spread.shape[1]), F32))
        left_ref[...] = jnp.concatenate(parts, axis=0).T[:out_rows, :total].astype(BF16)


def combine_kernel(*refs, members, slots, width, copies):
    count = len(members)
    full = slots * (width // LANES)
    sides, left_ref = refs[:count], refs[count]
    rest = refs[count + 1 :]
    before = None
    if copies:
        before, out_hbm, row_scr, tail_scr, out_ref, sems = rest
    else:
        out_ref, row_scr, tail_scr = rest
    n_main, n_tail = split_slots(slots)[1:]
    blocks = width // LANES
    per_half = n_tail * blocks
    padded = cdiv(count, SUB) * SUB
    first = lax.axis_index("tp") == 0
    if padded > count:
        tail_scr[...] = jnp.zeros_like(tail_scr)
    for b, ref in enumerate(sides):
        rows = slice(b * n_main, (b + 1) * n_main)
        whole = ref.shape[0] == full
        for j in range(0, blocks, 2):
            if whole:
                pair = [
                    ref[k * 2 * n_main : (k + 1) * 2 * n_main, :].astype(F32) for k in (j, j + 1)
                ]
                pair = [jnp.where(first, two[:n_main], two[n_main:]) for two in pair]
            else:
                two = ref[j * n_main : (j + 2) * n_main, :].astype(F32)
                pair = [two[:n_main], two[n_main:]]
            for k in range(2):
                row_scr[rows, (j + k) * LANES : (j + k + 1) * LANES] = pair[k]
        if whole:
            two = ref[2 * n_main * blocks :, :].astype(F32)
            two = jnp.where(first, two[:per_half], two[per_half:])
        else:
            two = ref[n_main * blocks :, :].astype(F32)
        tail_scr[b * per_half : (b + 1) * per_half, :] = two
    for t in range(n_tail):
        rows = slice(count * n_main + t * padded, count * n_main + (t + 1) * padded)
        for j in range(blocks):
            row_scr[rows, j * LANES : (j + 1) * LANES] = tail_scr[
                pl.ds(t * blocks + j, padded, stride=per_half), :
            ]
    left = left_ref[...]
    chunk = 2 * LANES
    started = []
    for at in range(0, width, chunk):
        cols = slice(at, at + chunk)
        rows = row_scr[:, cols].astype(BF16)
        got = jnp.dot(left, jnp.concatenate([rows] * 3, axis=0), preferred_element_type=F32)
        if before is not None:
            got = before[:, cols] + got
        out_ref[:, cols] = got.astype(out_ref.dtype)
        if copies and (at + chunk) % (width // copies) == 0:
            cols = slice(at + chunk - width // copies, at + chunk)
            started.append(
                pltpu.make_async_copy(
                    out_ref.at[:, cols], out_hbm.at[:, cols], sems.at[len(started)]
                )
            )
            started[-1].start()
    for copy in started:
        copy.wait()


def exchange(blocks, n_exp):
    far = len(blocks) - 1
    came, passed = [], []
    for m, block in enumerate(blocks):
        gap = [2 * (far - m) + turn(c, m) if m < far else 1 for c in range(2)]
        pairs = [(2 * e + c, 2 * (e ^ gap[c]) + c) for e in range(n_exp) for c in range(2)]
        came.append(lax.ppermute(block, ("ep", "tp"), pairs))
    for block in came[:far]:
        passed.append(lax.ppermute(block, "tp", SWAP))
    return came[:far], passed, came[far]


def local(tokens, norm_gain, chosen_rows, route_weights, gate_weight, up_weight, down_weight):
    tok_rows, width = tokens.shape
    n_exp, slots = chosen_rows.shape
    _, n_tail = split_slots(slots)[1:]
    far = n_exp // 2 - 1
    hidden = gate_weight.shape[2]
    blocks = width // LANES
    block = jax.ShapeDtypeStruct((slots * blocks, LANES), BF16)
    padded = cdiv(far + 2, SUB) * SUB
    args = (tokens, norm_gain.reshape(blocks, LANES), chosen_rows, route_weights)
    params = pltpu.CompilerParams(vmem_limit_bytes=VMEM_LIMIT)
    *outgoing, own, own_rows, own_weights = pl.pallas_call(
        functools.partial(dispatch_kernel, far=far),
        out_shape=[block] * (far + 2)
        + [jax.ShapeDtypeStruct(x.shape, x.dtype) for x in (chosen_rows, route_weights)],
        in_specs=[HBM] * 4,
        out_specs=[VMEM] * (far + 4),
        scratch_shapes=[
            pltpu.VMEM((tok_rows, width), BF16),
            pltpu.VMEM((blocks, LANES), BF16),
            pltpu.VMEM((tok_rows, width), BF16),
            pltpu.VMEM((padded * 2 * n_tail * blocks, LANES), F32),
            pltpu.VMEM((padded, slots), jnp.int32),
            pltpu.SemaphoreType.DMA((COPIES + 3,)),
        ],
        compiler_params=params,
        name="dispatch",
    )(*(pltpu.with_memory_space_constraint(x, pltpu.HBM) for x in args))
    out_rows = tok_rows // 2
    members = groups(far)
    depths = [depth(len(m), slots) for m in members]
    weight_bytes = 3 * 2 * width * hidden
    most = cdiv(len(members[0]), SUB) * SUB
    lefts = pl.pallas_call(
        functools.partial(route_kernel, far=far),
        out_shape=[jax.ShapeDtypeStruct((out_rows, 3 * d), BF16) for d in depths],
        in_specs=[VMEM] * 2,
        out_specs=[VMEM] * 2,
        scratch_shapes=[pltpu.VMEM((most, slots), jnp.int32), pltpu.VMEM((most, slots), F32)],
        compiler_params=params,
        cost_estimate=pl.CostEstimate(
            flops=COVER_FLOPS, bytes_accessed=weight_bytes, transcendentals=0
        ),
        name="route",
    )(own_rows, own_weights)
    mine, other, near = exchange(outgoing, n_exp)
    tails = n_exp * 2 * n_tail * blocks
    results = pl.pallas_call(
        functools.partial(expert_kernel, far=far, slots=slots),
        out_shape=[block] * (2 * far + 2),
        in_specs=[VMEM] * (2 * far + 5),
        out_specs=[VMEM] * (2 * far + 2),
        scratch_shapes=[
            pltpu.VMEM((n_exp * slots, width), BF16),
            pltpu.VMEM((n_exp * slots, hidden), BF16),
            pltpu.VMEM((tails, LANES), F32),
            pltpu.VMEM((tails, LANES), F32),
        ],
        compiler_params=params,
        name="expert",
    )(*mine, *other, near, own, gate_weight, up_weight, down_weight)
    came = []
    for part in results[: far + 1]:
        came.append(lax.ppermute(part, "tp", SWAP))

    def add(a, b):
        return (a.astype(F32) + b.astype(F32)).astype(BF16)

    summed = [add(a, b) for a, b in zip(results[far + 1 : -1], came)]
    half = slots // 2 * blocks
    neighbour, own = (add(results[-1][rows], came[-1][rows]) for rows in (slice(0, half), slice(half, None)))
    mine, other, near = exchange(summed + [neighbour], n_exp)
    sides = ([*mine, near, own], other)
    total = None
    for k, (blocks_in, left) in enumerate(zip(members, lefts)):
        final = k == len(members) - 1
        ins = [sides[side][m] for side, m in blocks_in] + [left] + ([] if total is None else [total])
        total = pl.pallas_call(
            functools.partial(
                combine_kernel,
                members=blocks_in,
                slots=slots,
                width=width,
                copies=OUT_COPIES if final else 0,
            ),
            out_shape=jax.ShapeDtypeStruct((out_rows, width), BF16 if final else F32),
            in_specs=[VMEM] * len(ins),
            out_specs=pl.BlockSpec(memory_space=pl.ANY) if final else VMEM,
            scratch_shapes=[
                pltpu.VMEM((depths[k], width), F32),
                pltpu.VMEM((cdiv(len(blocks_in), SUB) * SUB * n_tail * blocks, LANES), F32),
            ]
            + [pltpu.VMEM((out_rows, width), BF16), pltpu.SemaphoreType.DMA((OUT_COPIES,))] * final,
            compiler_params=params,
        )(*ins)
    return total


def solution(mesh):
    return jax.shard_map(
        local,
        mesh=mesh,
        in_specs=(
            P(("grp", "ep"), None),
            P(),
            P("grp", "ep"),
            P("grp", "ep"),
            P("ep", None, "tp"),
            P("ep", None, "tp"),
            P("ep", "tp", None),
        ),
        out_specs=P(("grp", "ep", "tp"), None),
        check_vma=False,
    )
```
